32 devices in a mesh: ra: 4 (over z), cb: 4 (over y, x), dp: 2 (over core).
Axes of the slice: x: 2, y: 2, z: 4, core: 2. Of those that a mesh axis runs over, the one named last changes fastest.
Arguments:
- tokens: bfloat16 [2048, 4096], P('dp', 'cb'), may hold values from -3000 to 3000
- norm_gain: float32 [4096], P('cb'), may hold values from 0.1 to 1.9
- norm_bias: float32 [4096], P('cb'), may hold values from -2 to 2
- gate_weight: float32 [4096, 11264], P('cb', 'ra'), may hold values from -0.09375 to 0.09375
- up_weight: float32 [4096, 11264], P('cb', 'ra'), may hold values from -0.09375 to 0.09375
- gate_scale: float32 [11264], P('ra'), may hold values from 0.5 to 2
- up_scale: float32 [11264], P('ra'), may hold values from 0.5 to 2
- down_weight: float32 [11264, 4096], P('ra', 'cb'), may hold values from -0.0546875 to 0.0546875
- down_scale: float32 [4096], P('cb'), may hold values from 0.5 to 8
- out_gain: float32 [4096], P('cb'), may hold values from 0.1 to 1.9
- out_bias: float32 [4096], P('cb'), may hold values from -2 to 2
Outputs:
- result: bfloat16 [2048, 4096], P(('dp', 'ra'), 'cb')
The draws below stay inside these ranges and needn't reach their ends.
All inputs are finite; a program needn't handle non-finite values.
Results may differ from the reference program's by a relative error of at most 0.018.
Values may be sent and summed in bfloat16 or wider, within the bound.
A program may use at most 128 MiB of HBM per device.

```python
import math
import jax
import jax.numpy as jnp
from jax import lax

D = 4096
FF = 11264
TOKENS = 2048


def draw_tokens(key, part):
    keys = jax.random.split(key, 3)
    base = jax.random.normal(keys[0], (TOKENS, D), jnp.float32)
    columns = jnp.exp(math.log(6.0) * jnp.arange(D, dtype=jnp.float32) / D)
    columns = columns * jnp.exp(jax.random.uniform(keys[1], (D,), jnp.float32, -0.35, 0.35))
    rows_scale = jnp.exp(jax.random.uniform(keys[2], (TOKENS, 1), jnp.float32, 0.0, math.log(10.0)))
    values = base * columns * rows_scale
    return values.astype(jnp.bfloat16)


def draw_down_scale(key, part):
    rising = jnp.exp(math.log(4.0) * jnp.arange(D, dtype=jnp.float32) / D)
    factor = jnp.exp(jax.random.uniform(key, (D,), jnp.float32, math.log(0.5), math.log(2.0)))
    return (rising * factor).astype(jnp.float32)


def level_of(own_key, extent, pieces, smallest, high):
    def one(dim, shards_of):
        heights = jax.random.uniform(jax.random.fold_in(jax.random.fold_in(own_key, 6), dim), (shards_of,), jnp.float32, smallest / len(pieces), high / len(pieces))
        return jnp.repeat(jnp.exp(heights), extent[dim] // shards_of).reshape((-1,) + (1,) * (len(extent) - dim - 1))

    gain = one(*pieces[0])
    for cut in pieces[1:]:
        gain = gain * one(*cut)
    return gain


def gaussian(stream_key, dims, deviation, limit, pieces=(), kind=jnp.bfloat16):
    result = jax.random.normal(stream_key, dims, jnp.float32) * deviation
    if len(pieces) > 0:
        result = level_of(stream_key, dims, pieces, -0.22, 0.18) * result
    return jnp.clip(result, min=-limit, max=limit).astype(kind)


def setup_inputs(seed: int = 0) -> dict:
    streams_of = jax.random.split(jax.random.key(seed), 12)
    tokens = draw_tokens(jax.random.fold_in(streams_of[11], 71), 0)
    norm_gain = jnp.clip(1.0 + 0.18 * jax.random.normal(streams_of[1], (D,), jnp.float32), 0.1, 1.9)
    norm_bias = gaussian(streams_of[2], (D,), 0.3, 2.0, ((0, 4),), jnp.float32)
    gate_weight = gaussian(streams_of[3], (D, FF), D ** -0.5, 0.09375, ((0, 4), (1, 4)), jnp.float32)
    up_weight = gaussian(streams_of[4], (D, FF), D ** -0.5, 0.09375, ((0, 4), (1, 4)), jnp.float32)
    gate_scale = jnp.clip(jnp.exp(math.log(2.0) - 1.3862944 * jax.random.uniform(streams_of[5], (FF,), jnp.float32) ** level_of(streams_of[5], (FF,), ((0, 4),), -0.2, 0.2)), 0.5, 2.0)
    up_scale = jnp.clip(jnp.exp(math.log(2.0) - 1.3862944 * jax.random.uniform(streams_of[6], (FF,), jnp.float32) ** level_of(streams_of[6], (FF,), ((0, 4),), -0.2, 0.2)), 0.5, 2.0)
    down_weight = gaussian(streams_of[7], (FF, D), FF ** -0.5, 0.0546875, ((0, 4), (1, 4)), jnp.float32)
    down_scale = draw_down_scale(jax.random.fold_in(streams_of[11], 71), 0)
    out_gain = jnp.clip(1.0 + 0.18 * jax.random.normal(streams_of[9], (D,), jnp.float32), 0.1, 1.9)
    out_bias = gaussian(streams_of[10], (D,), 0.3, 2.0, ((0, 4),), jnp.float32)
    return dict(tokens=tokens, norm_gain=norm_gain, norm_bias=norm_bias, gate_weight=gate_weight, up_weight=up_weight, gate_scale=gate_scale, up_scale=up_scale, down_weight=down_weight, down_scale=down_scale, out_gain=out_gain, out_bias=out_bias)


def standardize(values):
    mean = lax.optimization_barrier(jnp.mean(values, axis=1, keepdims=True))
    centred = values - mean
    spread = lax.optimization_barrier(jnp.mean(centred * centred, axis=1, keepdims=True))
    return centred * lax.rsqrt(spread + 1e-05)

def reference(tokens, norm_gain, norm_bias, gate_weight, up_weight, gate_scale, up_scale, down_weight, down_scale, out_gain, out_bias):
    normed = (standardize(tokens.astype(jnp.float32)) * norm_gain + norm_bias).astype(jnp.bfloat16)
    gate = jnp.dot(normed, gate_weight.astype(jnp.bfloat16), preferred_element_type=jnp.float32) * gate_scale
    up = jnp.dot(normed, up_weight.astype(jnp.bfloat16), preferred_element_type=jnp.float32) * up_scale
    hidden = (jax.nn.silu(gate) * up).astype(jnp.bfloat16)
    branch = jnp.dot(hidden, down_weight.astype(jnp.bfloat16), preferred_element_type=jnp.float32) * down_scale
    mixed = 0.5 * normed.astype(jnp.float32) + branch
    return (standardize(mixed) * out_gain + out_bias).astype(jnp.bfloat16)
```

```python
import jax
import jax.numpy as jnp
from jax import lax
from jax.experimental import pallas as pl
from jax.experimental.pallas import tpu as pltpu
from jax.sharding import PartitionSpec as P

MESH = pl.DeviceIdType.MESH
EPS = 1e-05
TILE = 256
LANE = 128
PIECES = 4
G = 4
F32 = jnp.float32
BF16 = jnp.bfloat16


def standardize(values):
    width = values.shape[1] * lax.axis_size("cb")
    total = lax.psum(jnp.sum(values, axis=1), "cb")
    mean = total / width
    centred = values - mean[:, None]
    spread = lax.psum(jnp.sum(centred * centred, axis=1), "cb") / width
    return centred * lax.rsqrt(spread + EPS)[:, None]


def plain(
    tokens,
    norm_gain,
    norm_bias,
    gate_weight,
    up_weight,
    gate_scale,
    up_scale,
    down_weight,
    down_scale,
    out_gain,
    out_bias,
):
    normed = (standardize(tokens.astype(F32)) * norm_gain + norm_bias).astype(BF16)
    gate_part = jnp.dot(normed, gate_weight.astype(BF16), preferred_element_type=F32)
    up_part = jnp.dot(normed, up_weight.astype(BF16), preferred_element_type=F32)
    gate_share, up_share = (
        lax.psum_scatter(part.astype(BF16), "cb", scatter_dimension=1, tiled=True).astype(F32)
        for part in (gate_part, up_part)
    )
    share = gate_share.shape[1]
    offset = lax.axis_index("cb") * share
    gate_cols = lax.dynamic_slice_in_dim(gate_scale, offset, share, 0)
    up_cols = lax.dynamic_slice_in_dim(up_scale, offset, share, 0)
    hidden_share = (jax.nn.silu(gate_share * gate_cols) * (up_share * up_cols)).astype(BF16)
    hidden = lax.all_gather(hidden_share, "cb", axis=1, tiled=True)
    own_rows = hidden.shape[0] // lax.axis_size("ra")
    part = jnp.dot(hidden, down_weight.astype(BF16), preferred_element_type=F32)
    branch = lax.psum_scatter(part, "ra", scatter_dimension=0, tiled=True) * down_scale
    own_normed = lax.dynamic_slice_in_dim(normed, lax.axis_index("ra") * own_rows, own_rows, 0)
    mixed = 0.5 * own_normed.astype(F32) + branch
    return (standardize(mixed) * out_gain + out_bias).astype(BF16)


def tiles_of(ff):
    wide = (ff // LANE + 3) // 4 * LANE
    narrow = ff // 2 - wide
    count = (wide + TILE - 1) // TILE
    both = []
    for t in range(count):
        off = t * TILE
        both.append(((off, min(TILE, wide - off)), (off, min(TILE, narrow - off))))
    return wide, narrow, both


def kernel(
    tok,
    ng,
    nb,
    gw,
    uw,
    gs,
    us,
    dw,
    down_scale,
    og,
    ob,
    out,
    stage,
    stage_d,
    wa,
    wb,
    sa,
    sb,
    xt,
    gb,
    la,
    lb,
    pa,
    pb,
    ca,
    cb,
    ra,
    rb,
    hid,
    wd,
    bp,
    zr,
    mix,
    ms,
    st,
    st2,
    stage_sem,
    stage_d_sem,
    tok_s,
    tok_r,
    z_s,
    z_r,
    gb_s,
    gb_r,
    w_s,
    w_r,
    f_s,
    f_r,
    c_s,
    c_r,
    h_s,
    h_r,
    bp_s,
    bp_r,
    st_s,
    st_r,
):
    rows, width = tok.shape
    ff = gw.shape[1]
    na, nbw, tiles = tiles_of(ff)
    nt = len(tiles)
    base_b = 2 * na
    part = rows // G
    half = part // 2
    piece = part // PIECES
    kh = width // 2
    full = float(width * G)

    b = lax.axis_index("cb")
    r = lax.axis_index("ra")
    p = lax.axis_index("dp")
    x = lax.rem(b, 2)
    y = b // 2
    to_x = {"cb": b + 1 - 2 * x}
    to_y = {"cb": b + 2 - 4 * y}
    to_d = {"cb": (G - 1) - b}
    twin = {"dp": 1 - p}
    sets = [r + 1 - 2 * lax.rem(r, 2), r + 2 - 4 * (r // 2), (G - 1) - r, r]
    to_z = [{"ra": s} for s in sets[:3]]

    barrier = pltpu.get_barrier_semaphore()
    greet = [to_x, to_y, to_d, twin] + to_z
    for peer in greet:
        pl.semaphore_signal(barrier, inc=1, device_id=peer, device_id_type=MESH)

    def at(start, size, align):
        return pl.ds(pl.multiple_of(start, align), size)

    def remote(src, dst, send, recv, peer):
        return pltpu.make_async_remote_copy(
            src_ref=src,
            dst_ref=dst,
            send_sem=send,
            recv_sem=recv,
            device_id=peer,
            device_id_type=MESH,
        )

    def a_cols(t, who):
        off, w = tiles[t][0]
        return at(who * na + off, w, LANE)

    def b_cols(t, who):
        off, w = tiles[t][1]
        return at(base_b + who * nbw + off, w, LANE)

    def load_send(kind, t):
        slot = t % 2
        src = (gw, uw)[kind % 2]
        cols = a_cols(t, 1 - x) if kind < 2 else b_cols(t, 1 - y)
        w = tiles[t][kind // 2][1]
        return pltpu.make_async_copy(
            src.at[at(p * kh, kh, kh), cols],
            stage.at[kind, pl.ds(slot * kh, kh), pl.ds(0, w)],
            stage_sem.at[kind, slot],
        )

    def load_own(kind, t):
        src = (gw, uw)[kind % 2]
        cols = a_cols(t, x) if kind < 2 else b_cols(t, y)
        w = tiles[t][kind // 2][1]
        return pltpu.make_async_copy(
            src.at[:, cols], stage.at[kind, :, pl.ds(0, w)], stage_sem.at[kind, 0]
        )

    def tile_rows(t):
        return pl.ds(pl.multiple_of(t * TILE, TILE), TILE)

    def load_d(t, slot):
        return pltpu.make_async_copy(dw.at[tile_rows(t), :], stage_d.at[slot], stage_d_sem.at[slot])

    for t in range(min(2, nt)):
        for kind in range(4):
            load_send(kind, t).start()
    for t in range(2):
        load_d(t, t).start()

    pl.semaphore_wait(barrier, len(greet))

    own_tok = []
    for i in range(PIECES):
        rows_i = at(r * part + i * piece, piece, piece)
        for j, peer in enumerate((to_x, to_y)):
            own_tok.append(
                remote(tok.at[rows_i, :], xt.at[j, rows_i, :], tok_s.at[j, i], tok_r.at[j, i], peer)
            )
    for copy in own_tok:
        copy.start()
    gains = []
    for j, peer in enumerate((to_x, to_y)):
        for i, ref in enumerate((ng, nb)):
            gains.append(remote(ref, gb.at[j, i], gb_s.at[j, i], gb_r.at[j, i], peer))
    for copy in gains:
        copy.start()

    wcopy = {}
    fcopy = {}
    for t in range(nt):
        for s in range(2):
            off, w = tiles[t][s]
            mine = (sa, sb)[s].at[:, :, pl.ds(off, w)]
            there = (wa, wb)[s].at[:, at(width + p * kh, kh, kh), pl.ds(off, w)]
            wcopy[t, s] = remote(mine, there, w_s.at[t, s], w_r.at[t, s], (to_x, to_y)[s])
            fcopy[t, s] = remote(there, there, f_s.at[t, s], f_r.at[t, s], twin)

    def send_weights(t):
        for kind in range(4):
            load_send(kind, t).wait()
            s, g = kind // 2, kind % 2
            off, w = tiles[t][s]
            (sa, sb)[s][g, :, off : off + w] = stage[kind, (t % 2) * kh : (t % 2 + 1) * kh, 0:w].astype(BF16)
            if t + 2 < nt:
                load_send(kind, t + 2).start()
        for s in range(2):
            wcopy[t, s].start()

    def put_stats(v, dst, col):
        total = jnp.sum(v, axis=1, keepdims=True)
        off = v - total * (1.0 / width)
        spread = jnp.sum(off * off, axis=1, keepdims=True)
        lane = lax.broadcasted_iota(jnp.int32, (v.shape[0], LANE), 1)
        both = jnp.where(lane == 0, total, spread)
        dst[0, :, pl.ds(col, v.shape[0])] = both.T[:8, :]

    def get_stats(src, col, n):
        parts = [src[i, 0:2, pl.ds(col, n)] for i in range(G)]
        mean = (parts[0][0:1] + parts[1][0:1] + parts[2][0:1] + parts[3][0:1]) / full
        spread = jnp.zeros_like(mean)
        for q in parts:
            d = q[0:1] * (1.0 / width) - mean
            spread = spread + q[1:2] + width * (d * d)
        inv = lax.rsqrt(spread / full + EPS)
        sub = lax.broadcasted_iota(jnp.int32, (LANE, n), 0)
        return jnp.where(sub == 0, mean, inv).T

    def swap_stats(buf, which):
        return [
            remote(buf.at[0], buf.at[1 + i], st_s.at[which, i], st_r.at[which, i], peer)
            for i, peer in enumerate((to_x, to_y, to_d))
        ]

    send_weights(0)
    for j in range(G):
        put_stats(tok[pl.ds(j * part, part), :].astype(F32), st, j * part)
    swap1 = swap_stats(st, 0)
    for copy in swap1:
        copy.start()

    def zcopy(way, dist, j, i):
        q = r - dist if way == 0 else r + dist
        rows_q = at(q * part + i * piece, piece, piece)
        ref = xt.at[j, rows_q, :]
        peer = {"ra": r + 1 if way == 0 else r - 1}
        return remote(ref, ref, z_s.at[way, dist, j, i], z_r.at[way, dist, j, i], peer)

    def spread_own(i):
        for j in range(2):
            own_tok[2 * i + j].wait_recv()
        for way in range(2):

            @pl.when((r < G - 1) if way == 0 else (r > 0))
            def _():
                for j in range(2):
                    zcopy(way, 0, j, i).start()

    def arrive(dist, i):
        for way in range(2):

            @pl.when((r >= dist) if way == 0 else (r <= G - 1 - dist))
            def _():
                q = r - dist if way == 0 else r + dist
                rows_q = at(q * part + i * piece, piece, piece)
                for j in range(2):
                    ref = xt.at[j, rows_q, :]
                    remote(
                        ref, ref, z_s.at[way, dist - 1, j, i], z_r.at[way, dist - 1, j, i], to_x
                    ).wait_recv()

            if dist < G - 1:

                @pl.when(
                    jnp.logical_and(r >= dist, r < G - 1)
                    if way == 0
                    else jnp.logical_and(r <= G - 1 - dist, r > 0)
                )
                def _():
                    for j in range(2):
                        zcopy(way, dist, j, i).start()

    for t in range(1, nt):
        send_weights(t)
    for kind in range(4):
        load_own(kind, 0).start()

    spread_own(0)
    spread_own(1)
    for t in range(nt):
        for kind in range(4):
            load_own(kind, t).wait()
            s, g = kind // 2, kind % 2
            off, w = tiles[t][s]
            (wa, wb)[s][g, 0:width, off : off + w] = stage[kind, :, 0:w].astype(BF16)
            if t + 1 < nt:
                load_own(kind, t + 1).start()
    spread_own(2)
    for copy in swap1:
        copy.wait_recv()
    for j in range(G):
        ms[pl.ds(j * part, part), :] = get_stats(st, j * part, part)
    spread_own(3)
    for copy in gains:
        copy.wait_recv()

    def cast_d(t, carry):
        slot = lax.rem(t, 2)
        load_d(t, slot).wait()
        wd[tile_rows(t), :] = stage_d[slot].astype(BF16)

        @pl.when(t + 2 < ff // TILE)
        def _():
            load_d(t + 2, slot).start()

        return carry

    lax.fori_loop(0, ff // TILE, cast_d, 0)

    def normalize(k):
        for i in range(2):
            rows_i = at(sets[k] * part + i * half, half, half)
            both = ms[rows_i, :]
            mean, inv = both[:, 0:1], both[:, 1:2]

            def norm(v, gain, bias):
                return ((v.astype(F32) - mean) * inv * gain + bias).astype(BF16)

            for lhs, j, side in ((la, 0, y), (lb, 1, x)):
                spot = at((i + side - 2 * i * side) * half, half, half)
                lhs[spot, 0:width] = norm(tok[rows_i, :], ng[...], nb[...])
                lhs[spot, width : 2 * width] = norm(xt[j, rows_i, :], gb[j, 0], gb[j, 1])

    ccopy = {}
    hcopy = {}
    for k in range(G):
        for t in range(nt):
            m = k * nt + t
            spot = pl.ds(k * half, half)
            for s in range(2):
                off, w = tiles[t][s]
                region = (ca, cb)[s].at[:, spot, pl.ds(off, w)]
                land = (ra, rb)[s].at[:, spot, pl.ds(off, w)]
                ccopy[m, s] = remote(region, land, c_s.at[s, m], c_r.at[s, m], (to_y, to_x)[s])
                side, who = ((y, x), (x, y))[s]
                cols = (a_cols, b_cols)[s]

                def block(side_, who_, lo, n):
                    return hid.at[at(sets[k] * part + side_ * half + lo, n, n), cols(t, who_)]

                own = block(side, who, 0, half)
                of_x = block(side, 1 - who, 0, half // 2) if s == 0 else block(1 - side, who, 0, half // 2)
                of_y = (
                    block(1 - side, who, half // 2, half // 2)
                    if s == 0
                    else block(side, 1 - who, half // 2, half // 2)
                )
                hcopy[m, s] = [
                    remote(own, own, h_s.at[s, 0, m], h_r.at[s, 0, m], to_x),
                    remote(own, own, h_s.at[s, 1, m], h_r.at[s, 1, m], to_y),
                    remote(of_x, of_x, h_s.at[s, 2, m], h_r.at[s, 2, m], to_y),
                    remote(of_y, of_y, h_s.at[s, 3, m], h_r.at[s, 3, m], to_x),
                ]

    def s1(m):
        k, t = m // nt, m % nt
        for s in range(2):
            off, w = tiles[t][s]
            lhs, wgt, keep, away = ((la, wa, pa, ca), (lb, wb, pb, cb))[s]

            def one(g, carry):
                acc = jnp.dot(lhs[...], wgt[g, :, off : off + w], preferred_element_type=F32)
                keep[g, k * half : (k + 1) * half, off : off + w] = acc[:half]
                away[g, k * half : (k + 1) * half, off : off + w] = acc[half:].astype(BF16)
                return carry

            lax.fori_loop(0, 2, one, 0)
            ccopy[m, s].start()

    def s2(m):
        k, t = m // nt, m % nt
        for s in range(2):
            ccopy[m, s].wait_recv()
            off, w = tiles[t][s]
            keep, got = ((pa, ra), (pb, rb))[s]
            side, who = ((y, x), (x, y))[s]
            cols = (a_cols, b_cols)[s](t, who)
            spot = pl.ds(k * half, half)
            g = keep[0, spot, off : off + w] + got[0, spot, off : off + w].astype(F32)
            u = keep[1, spot, off : off + w] + got[1, spot, off : off + w].astype(F32)
            g = g * gs[:, cols]
            u = u * us[:, cols]
            h = (g / (1.0 + jnp.exp(-g)) * u).astype(BF16)
            hid[at(sets[k] * part + side * half, half, half), cols] = h
            hcopy[m, s][0].start()
            hcopy[m, s][1].start()

    def s3(m):
        for s in range(2):
            hcopy[m, s][0].wait_recv()
            hcopy[m, s][2].start()
            hcopy[m, s][1].wait_recv()
            hcopy[m, s][3].start()

    zcp = [remote(bp.at[k], zr.at[k], bp_s.at[k], bp_r.at[k], to_z[k]) for k in range(G - 1)]

    def s4(k):
        for t in range(nt):
            for s in range(2):
                for i in (2, 3):
                    hcopy[k * nt + t, s][i].wait_recv()
        lhs = at(sets[k] * part, part, part)
        if k == G - 1:
            for copy in zcp:
                copy.wait_recv()

        def body(n, carry):
            cols = pl.ds(pl.multiple_of(n * TILE, TILE), TILE)
            acc = jnp.dot(hid[lhs, :], wd[:, cols], preferred_element_type=F32)
            if k < G - 1:
                bp[k, :, cols] = acc.astype(BF16)
            else:
                for q in range(G - 1):
                    acc = acc + zr[q, :, cols].astype(F32)
                acc = acc * down_scale[:, cols]
                for i in range(2):
                    spot = at((i + y - 2 * i * y) * half, half, half)
                    mix[i * half : (i + 1) * half, cols] = (
                        0.5 * la[spot, cols].astype(F32) + acc[i * half : (i + 1) * half]
                    )
            return carry

        lax.fori_loop(0, width // TILE, body, 0)
        if k < G - 1:
            zcp[k].start()

    def weights_in(t):
        for s in range(2):
            wcopy[t, s].wait_recv()
            fcopy[t, s].start()

    def weights_ready(t):
        for s in range(2):
            fcopy[t, s].wait_recv()

    for i in range(PIECES // 2):
        arrive(1, i)
    weights_in(0)
    for i in range(PIECES // 2, PIECES):
        arrive(1, i)
    normalize(0)
    weights_ready(0)

    steps = G * nt
    for i in range(steps + 4):
        if 0 < i < nt:
            weights_in(i)
            weights_ready(i)
        if i == nt:
            for j in range(PIECES):
                arrive(2, j)
        if i == 2 * nt:
            for j in range(PIECES):
                arrive(3, j)
        if i % nt == 0 and 0 < i < steps:
            normalize(i // nt)
        if i < steps:
            s1(i)
        if 0 <= i - 2 < steps:
            s2(i - 2)
        if 0 <= i - 3 < steps:
            s3(i - 3)
        if i - 4 >= 0 and (i - 4) % nt == nt - 1:
            s4((i - 4) // nt)

    put_stats(mix[...], st2, 0)
    swap2 = swap_stats(st2, 1)
    for copy in swap2:
        copy.start()
    for copy in swap2:
        copy.wait_recv()
    both = get_stats(st2, 0, part)
    out[...] = ((mix[...] - both[:, 0:1]) * both[:, 1:2] * og[...] + ob[...]).astype(BF16)

    for copy in swap1 + swap2 + own_tok + gains + zcp:
        copy.wait_send()
    for group in (wcopy, fcopy, ccopy):
        for copy in group.values():
            copy.wait_send()
    for group in hcopy.values():
        for copy in group:
            copy.wait_send()
    for way in range(2):
        for dist in range(G - 1):

            @pl.when(
                jnp.logical_and(r >= dist, r < G - 1)
                if way == 0
                else jnp.logical_and(r <= G - 1 - dist, r > 0)
            )
            def _():
                for i in range(PIECES):
                    for j in range(2):
                        zcopy(way, dist, j, i).wait_send()


def fused(
    tokens,
    norm_gain,
    norm_bias,
    gate_weight,
    up_weight,
    gate_scale,
    up_scale,
    down_weight,
    down_scale,
    out_gain,
    out_bias,
):
    rows, width = tokens.shape
    ff = gate_weight.shape[1]
    na, nbw, tiles = tiles_of(ff)
    nt = len(tiles)
    part = rows // G
    half = part // 2
    kh = width // 2
    steps = G * nt
    vmem = pl.BlockSpec(memory_space=pltpu.VMEM)
    hbm = pl.BlockSpec(memory_space=pl.ANY)
    row = lambda v: v.reshape(1, -1)
    dma = pltpu.SemaphoreType.DMA
    return pl.pallas_call(
        kernel,
        out_shape=jax.ShapeDtypeStruct((part, width), BF16),
        in_specs=[vmem, vmem, vmem, hbm, hbm, vmem, vmem, hbm, vmem, vmem, vmem],
        out_specs=vmem,
        scratch_shapes=[
            pltpu.VMEM((4, width, TILE), F32),
            pltpu.VMEM((2, TILE, width), F32),
            pltpu.VMEM((2, 2 * width, na), BF16),
            pltpu.VMEM((2, 2 * width, nbw), BF16),
            pltpu.VMEM((2, kh, na), BF16),
            pltpu.VMEM((2, kh, nbw), BF16),
            pltpu.VMEM((2, rows, width), BF16),
            pltpu.VMEM((2, 2, 1, width), F32),
            pltpu.VMEM((part, 2 * width), BF16),
            pltpu.VMEM((part, 2 * width), BF16),
            pltpu.VMEM((2, rows // 2, na), F32),
            pltpu.VMEM((2, rows // 2, nbw), F32),
            pltpu.VMEM((2, rows // 2, na), BF16),
            pltpu.VMEM((2, rows // 2, nbw), BF16),
            pltpu.VMEM((2, rows // 2, na), BF16),
            pltpu.VMEM((2, rows // 2, nbw), BF16),
            pltpu.VMEM((rows, ff), BF16),
            pltpu.VMEM((ff, width), BF16),
            pltpu.VMEM((G - 1, part, width), BF16),
            pltpu.VMEM((G - 1, part, width), BF16),
            pltpu.VMEM((part, width), F32),
            pltpu.VMEM((rows, LANE), F32),
            pltpu.VMEM((G, 8, rows), F32),
            pltpu.VMEM((G, 8, part), F32),
            dma((4, 2)),
            dma((2,)),
            dma((2, PIECES)),
            dma((2, PIECES)),
            dma((2, G - 1, 2, PIECES)),
            dma((2, G - 1, 2, PIECES)),
            dma((2, 2)),
            dma((2, 2)),
            dma((nt, 2)),
            dma((nt, 2)),
            dma((nt, 2)),
            dma((nt, 2)),
            dma((2, steps)),
            dma((2, steps)),
            dma((2, 4, steps)),
            dma((2, 4, steps)),
            dma((G - 1,)),
            dma((G - 1,)),
            dma((2, G - 1)),
            dma((2, G - 1)),
        ],
        compiler_params=pltpu.CompilerParams(
            collective_id=0, has_side_effects=True, vmem_limit_bytes=67043328
        ),
    )(
        tokens,
        row(norm_gain),
        row(norm_bias),
        gate_weight,
        up_weight,
        row(gate_scale),
        row(up_scale),
        down_weight,
        row(down_scale),
        row(out_gain),
        row(out_bias),
    )


def local(*args):
    rows, width = args[0].shape
    ff = args[3].shape[1]
    fits = (
        lax.axis_size("cb") == G
        and lax.axis_size("ra") == G
        and lax.axis_size("dp") == 2
        and rows % (256 * G) == 0
        and width % TILE == 0
        and ff % TILE == 0
        and min(pair[1][1] for pair in tiles_of(ff)[2]) > 0
        and rows * width <= 1 << 20
        and ff * width <= 2816 * 1024
    )
    return (fused if fits else plain)(*args)


def solution(mesh):
    return jax.shard_map(
        local,
        mesh=mesh,
        in_specs=(
            P("dp", "cb"),
            P("cb"),
            P("cb"),
            P("cb", "ra"),
            P("cb", "ra"),
            P("ra"),
            P("ra"),
            P("ra", "cb"),
            P("cb"),
            P("cb"),
            P("cb"),
        ),
        out_specs=P(("dp", "ra"), "cb"),
        check_vma=False,
    )
```

```python
import jax
import jax.numpy as jnp
from jax import lax
from jax.experimental import pallas as pl
from jax.experimental.pallas import tpu as pltpu
from jax.sharding import PartitionSpec as P

MESH = pl.DeviceIdType.MESH
EPS = 1e-05
TILE = 256
LANE = 128
PIECES = 4
SKEW = (1, 2, 3)
G = 4
F32 = jnp.float32
BF16 = jnp.bfloat16


def standardize(values):
    width = values.shape[1] * lax.axis_size("cb")
    total = lax.psum(jnp.sum(values, axis=1), "cb")
    mean = total / width
    centred = values - mean[:, None]
    spread = lax.psum(jnp.sum(centred * centred, axis=1), "cb") / width
    return centred * lax.rsqrt(spread + EPS)[:, None]


def plain(
    tokens,
    norm_gain,
    norm_bias,
    gate_weight,
    up_weight,
    gate_scale,
    up_scale,
    down_weight,
    down_scale,
    out_gain,
    out_bias,
):
    normed = (standardize(tokens.astype(F32)) * norm_gain + norm_bias).astype(BF16)
    gate_part = jnp.dot(normed, gate_weight.astype(BF16), preferred_element_type=F32)
    up_part = jnp.dot(normed, up_weight.astype(BF16), preferred_element_type=F32)
    gate_share, up_share = (
        lax.psum_scatter(part.astype(BF16), "cb", scatter_dimension=1, tiled=True).astype(F32)
        for part in (gate_part, up_part)
    )
    share = gate_share.shape[1]
    offset = lax.axis_index("cb") * share
    gate_cols = lax.dynamic_slice_in_dim(gate_scale, offset, share, 0)
    up_cols = lax.dynamic_slice_in_dim(up_scale, offset, share, 0)
    hidden_share = (jax.nn.silu(gate_share * gate_cols) * (up_share * up_cols)).astype(BF16)
    hidden = lax.all_gather(hidden_share, "cb", axis=1, tiled=True)
    own_rows = hidden.shape[0] // lax.axis_size("ra")
    part = jnp.dot(hidden, down_weight.astype(BF16), preferred_element_type=F32)
    branch = lax.psum_scatter(part, "ra", scatter_dimension=0, tiled=True) * down_scale
    own_normed = lax.dynamic_slice_in_dim(normed, lax.axis_index("ra") * own_rows, own_rows, 0)
    mixed = 0.5 * own_normed.astype(F32) + branch
    return (standardize(mixed) * out_gain + out_bias).astype(BF16)


def tiles_of(ff):
    wide = (ff // LANE + 3) // 4 * LANE
    narrow = ff // 2 - wide
    count = (wide + TILE - 1) // TILE
    both = []
    for t in range(count):
        off = t * TILE
        both.append(((off, min(TILE, wide - off)), (off, min(TILE, narrow - off))))
    return wide, narrow, both


def kernel(
    tok_hbm,
    ng_hbm,
    nb_hbm,
    gw,
    uw,
    gs_hbm,
    us_hbm,
    dw,
    ds_hbm,
    og_hbm,
    ob_hbm,
    out_hbm,
    tok,
    ng,
    nb,
    gs,
    us,
    down_scale,
    og,
    ob,
    out,
    stage,
    stage_d,
    wa,
    wb,
    sa,
    sb,
    xt,
    gb,
    la,
    lb,
    pa,
    pb,
    ca,
    cb,
    ra,
    rb,
    hid,
    wd,
    bp,
    zr,
    zs,
    mix,
    ms,
    st,
    st2,
    in_sem,
    out_sem,
    stage_sem,
    stage_d_sem,
    tok_s,
    tok_r,
    z_s,
    z_r,
    gb_s,
    gb_r,
    w_s,
    w_r,
    f_s,
    f_r,
    c_s,
    c_r,
    h_s,
    h_r,
    bp_s,
    bp_r,
    zs_r,
    st_s,
    st_r,
):
    rows, width = tok.shape
    ff = gw.shape[1]
    na, nbw, tiles = tiles_of(ff)
    nt = len(tiles)
    base_b = 2 * na
    part = rows // G
    half = part // 2
    piece = part // PIECES
    kh = width // 2
    full = float(width * G)

    b = lax.axis_index("cb")
    r = lax.axis_index("ra")
    p = lax.axis_index("dp")
    x = lax.rem(b, 2)
    y = b // 2
    to_x = {"cb": b + 1 - 2 * x}
    to_y = {"cb": b + 2 - 4 * y}
    to_d = {"cb": (G - 1) - b}
    twin = {"dp": 1 - p}
    hi = r // 2
    sets = [3 - 3 * hi, 2 - hi, r + 1 - 2 * lax.rem(r, 2), r]
    inner = lax.rem(r, 2) + hi == 1
    to_z = [{"ra": s} for s in sets[:3]]
    ring = [{"ra": lax.rem(r + o, G)} for o in range(1, G)]

    barrier = pltpu.get_barrier_semaphore()
    greet = [to_x, to_y, to_d, twin] + ring
    for peer in greet:
        pl.semaphore_signal(barrier, inc=1, device_id=peer, device_id_type=MESH)

    small = [
        pltpu.make_async_copy(src, dst, in_sem.at[G + i])
        for i, (src, dst) in enumerate(
            (
                (ng_hbm, ng),
                (nb_hbm, nb),
                (gs_hbm, gs),
                (us_hbm, us),
                (ds_hbm, down_scale),
                (og_hbm, og),
                (ob_hbm, ob),
            )
        )
    ]
    tok_in = [
        pltpu.make_async_copy(
            tok_hbm.at[pl.ds(j * part, part), :], tok.at[pl.ds(j * part, part), :], in_sem.at[j]
        )
        for j in range(G)
    ]
    for copy in tok_in + small:
        copy.start()

    def at(start, size, align):
        return pl.ds(pl.multiple_of(start, align), size)

    def remote(src, dst, send, recv, peer):
        return pltpu.make_async_remote_copy(
            src_ref=src,
            dst_ref=dst,
            send_sem=send,
            recv_sem=recv,
            device_id=peer,
            device_id_type=MESH,
        )

    def a_cols(t, who):
        off, w = tiles[t][0]
        return at(who * na + off, w, LANE)

    def b_cols(t, who):
        off, w = tiles[t][1]
        return at(base_b + who * nbw + off, w, LANE)

    def load_send(kind, t):
        slot = t % 2
        src = (gw, uw)[kind % 2]
        cols = a_cols(t, 1 - x) if kind < 2 else b_cols(t, 1 - y)
        w = tiles[t][kind // 2][1]
        return pltpu.make_async_copy(
            src.at[at(p * kh, kh, kh), cols],
            stage.at[kind, pl.ds(slot * kh, kh), pl.ds(0, w)],
            stage_sem.at[kind, slot],
        )

    def load_own(kind, t):
        src = (gw, uw)[kind % 2]
        cols = a_cols(t, x) if kind < 2 else b_cols(t, y)
        w = tiles[t][kind // 2][1]
        return pltpu.make_async_copy(
            src.at[:, cols], stage.at[kind, :, pl.ds(0, w)], stage_sem.at[kind, 0]
        )

    def tile_rows(t):
        return pl.ds(pl.multiple_of(t * TILE, TILE), TILE)

    def load_d(t, slot):
        return pltpu.make_async_copy(dw.at[tile_rows(t), :], stage_d.at[slot], stage_d_sem.at[slot])

    for t in range(min(2, nt)):
        for kind in range(4):
            load_send(kind, t).start()
    for t in range(2):
        load_d(t, t).start()

    def put_stats(v, dst, col):
        total = jnp.sum(v, axis=1, keepdims=True)
        off = v - total * (1.0 / width)
        spread = jnp.sum(off * off, axis=1, keepdims=True)
        lane = lax.broadcasted_iota(jnp.int32, (v.shape[0], LANE), 1)
        both = jnp.where(lane == 0, total, spread)
        dst[0, :, pl.ds(col, v.shape[0])] = both.T[:8, :]

    def get_stats(src, col, n):
        parts = [src[i, 0:2, pl.ds(col, n)] for i in range(G)]
        mean = (parts[0][0:1] + parts[1][0:1] + parts[2][0:1] + parts[3][0:1]) / full
        spread = jnp.zeros_like(mean)
        for q in parts:
            d = q[0:1] * (1.0 / width) - mean
            spread = spread + q[1:2] + width * (d * d)
        inv = lax.rsqrt(spread / full + EPS)
        sub = lax.broadcasted_iota(jnp.int32, (LANE, n), 0)
        return jnp.where(sub == 0, mean, inv).T

    def swap_stats(buf, which):
        return [
            remote(buf.at[0, pl.ds(0, 2)], buf.at[1 + i, pl.ds(0, 2)], st_s.at[which, i], st_r.at[which, i], peer)
            for i, peer in enumerate((to_x, to_y, to_d))
        ]

    for j in range(G):
        tok_in[j].wait()
        put_stats(tok[pl.ds(j * part, part), :].astype(F32), st, j * part)
    for copy in small:
        copy.wait()
    pl.semaphore_wait(barrier, len(greet))

    swap1 = swap_stats(st, 0)
    for copy in swap1:
        copy.start()

    own_tok = []
    for i in range(PIECES):
        rows_i = at((G - 1 - r) * part + i * piece, piece, piece)
        for j, peer in enumerate((to_x, to_y)):
            own_tok.append(
                remote(tok.at[rows_i, :], xt.at[j, rows_i, :], tok_s.at[j], tok_r.at[j, i], peer)
            )
    for copy in own_tok:
        copy.start()
    gains = []
    for j, peer in enumerate((to_x, to_y)):
        for i, ref in enumerate((ng, nb)):
            gains.append(remote(ref, gb.at[j, i], gb_s.at[j, i], gb_r.at[j, i], peer))
    for copy in gains:
        copy.start()

    wcopy = {}
    fcopy = {}
    for t in range(nt):
        for s in range(2):
            off, w = tiles[t][s]
            mine = (sa, sb)[s].at[:, :, pl.ds(off, w)]
            there = (wa, wb)[s].at[:, at(width + p * kh, kh, kh), pl.ds(off, w)]
            wcopy[t, s] = remote(mine, there, w_s.at[s], w_r.at[t, s], (to_x, to_y)[s])
            fcopy[t, s] = remote(there, there, f_s.at[s], f_r.at[t, s], twin)

    def send_weights(t):
        for kind in range(4):
            load_send(kind, t).wait()
            s, g = kind // 2, kind % 2
            off, w = tiles[t][s]
            (sa, sb)[s][g, :, off : off + w] = stage[kind, (t % 2) * kh : (t % 2 + 1) * kh, 0:w].astype(BF16)
            if t + 2 < nt:
                load_send(kind, t + 2).start()
        for s in range(2):
            wcopy[t, s].start()

    def zcopy(way, dist, j, i):
        q = r - dist if way == 0 else r + dist
        rows_q = at((G - 1 - q) * part + i * piece, piece, piece)
        ref = xt.at[j, rows_q, :]
        peer = {"ra": r + 1 if way == 0 else r - 1}
        return remote(ref, ref, z_s.at[way, dist], z_r.at[way, dist, j, i], peer)

    def spread_own(i):
        for j in range(2):
            own_tok[2 * i + j].wait_recv()
        for way in range(2):

            @pl.when((r < G - 1) if way == 0 else (r > 0))
            def _():
                for j in range(2):
                    zcopy(way, 0, j, i).start()

    def arrive(dist, i):
        for way in range(2):

            @pl.when((r >= dist) if way == 0 else (r <= G - 1 - dist))
            def _():
                q = r - dist if way == 0 else r + dist
                rows_q = at((G - 1 - q) * part + i * piece, piece, piece)
                for j in range(2):
                    ref = xt.at[j, rows_q, :]
                    remote(
                        ref, ref, z_s.at[way, dist - 1], z_r.at[way, dist - 1, j, i], to_x
                    ).wait_recv()

            if dist < G - 1:

                @pl.when(
                    jnp.logical_and(r >= dist, r < G - 1)
                    if way == 0
                    else jnp.logical_and(r <= G - 1 - dist, r > 0)
                )
                def _():
                    for j in range(2):
                        zcopy(way, dist, j, i).start()

    for t in range(nt):
        send_weights(t)
    for kind in range(4):
        load_own(kind, 0).start()

    spread_own(0)
    spread_own(1)
    for t in range(nt):
        for kind in range(4):
            load_own(kind, t).wait()
            s, g = kind // 2, kind % 2
            off, w = tiles[t][s]
            (wa, wb)[s][g, 0:width, off : off + w] = stage[kind, :, 0:w].astype(BF16)
            if t + 1 < nt:
                load_own(kind, t + 1).start()
    spread_own(2)
    for copy in swap1:
        copy.wait_recv()
    for j in range(G):
        ms[pl.ds(j * part, part), :] = get_stats(st, j * part, part)
    spread_own(3)
    for copy in gains:
        copy.wait_recv()

    def cast_d(t, carry):
        slot = lax.rem(t, 2)
        load_d(t, slot).wait()
        wd[tile_rows(t), :] = stage_d[slot].astype(BF16)

        @pl.when(t + 2 < ff // TILE)
        def _():
            load_d(t + 2, slot).start()

        return carry

    lax.fori_loop(0, ff // TILE, cast_d, 0)

    def normalize(k):
        for i in range(2):
            rows_i = at(sets[k] * part + i * half, half, half)
            both = ms[rows_i, :]
            mean, inv = both[:, 0:1], both[:, 1:2]

            def norm(v, gain, bias):
                return ((v.astype(F32) - mean) * inv * gain + bias).astype(BF16)

            for lhs, j, side in ((la, 0, y), (lb, 1, x)):
                spot = at((i + side - 2 * i * side) * half, half, half)
                lhs[spot, 0:width] = norm(tok[rows_i, :], ng[...], nb[...])
                lhs[spot, width : 2 * width] = norm(xt[j, rows_i, :], gb[j, 0], gb[j, 1])

    ccopy = {}
    hcopy = {}
    for k in range(G):
        for t in range(nt):
            m = k * nt + t
            spot = pl.ds(k * half, half)
            for s in range(2):
                off, w = tiles[t][s]
                region = (ca, cb)[s].at[:, spot, pl.ds(off, w)]
                land = (ra, rb)[s].at[:, spot, pl.ds(off, w)]
                ccopy[m, s] = remote(region, land, c_s.at[s], c_r.at[s, m], (to_y, to_x)[s])
                side, who = ((y, x), (x, y))[s]
                cols = (a_cols, b_cols)[s]

                def block(side_, who_, lo, n):
                    return hid.at[at(sets[k] * part + side_ * half + lo, n, n), cols(t, who_)]

                own = block(side, who, 0, half)
                of_x = block(side, 1 - who, 0, half // 2) if s == 0 else block(1 - side, who, 0, half // 2)
                of_y = (
                    block(1 - side, who, half // 2, half // 2)
                    if s == 0
                    else block(side, 1 - who, half // 2, half // 2)
                )
                hcopy[m, s] = [
                    remote(own, own, h_s.at[s, 0], h_r.at[s, 0, m], to_x),
                    remote(own, own, h_s.at[s, 1], h_r.at[s, 1, m], to_y),
                    remote(of_x, of_x, h_s.at[s, 2], h_r.at[s, 2, m], to_y),
                    remote(of_y, of_y, h_s.at[s, 3], h_r.at[s, 3, m], to_x),
                ]

    def scale_row(ref, s, t, who):
        off, w = tiles[t][s]
        first = (s * base_b + who * (na, nbw)[s] + off) // LANE
        return jnp.concatenate([ref[pl.ds(first + i, 1), :] for i in range(w // LANE)], axis=1)

    def s1(m):
        k, t = m // nt, m % nt
        for s in range(2):
            off, w = tiles[t][s]
            lhs, wgt, keep, away = ((la, wa, pa, ca), (lb, wb, pb, cb))[s]

            def one(g, carry):
                acc = jnp.dot(lhs[...], wgt[g, :, off : off + w], preferred_element_type=F32)
                keep[g, k * half : (k + 1) * half, off : off + w] = acc[:half]
                away[g, k * half : (k + 1) * half, off : off + w] = acc[half:].astype(BF16)
                return carry

            lax.fori_loop(0, 2, one, 0)
            ccopy[m, s].start()

    def s2(m):
        k, t = m // nt, m % nt
        for s in range(2):
            ccopy[m, s].wait_recv()
            off, w = tiles[t][s]
            keep, got = ((pa, ra), (pb, rb))[s]
            side, who = ((y, x), (x, y))[s]
            cols = (a_cols, b_cols)[s](t, who)
            spot = pl.ds(k * half, half)
            g = keep[0, spot, off : off + w] + got[0, spot, off : off + w].astype(F32)
            u = keep[1, spot, off : off + w] + got[1, spot, off : off + w].astype(F32)
            g = g * scale_row(gs, s, t, who)
            u = u * scale_row(us, s, t, who)
            h = (g / (1.0 + jnp.exp(-g)) * u).astype(BF16)
            hid[at(sets[k] * part + side * half, half, half), cols] = h
            hcopy[m, s][0].start()
            hcopy[m, s][1].start()

    def s3(m):
        for s in range(2):
            hcopy[m, s][0].wait_recv()
            hcopy[m, s][2].start()
            hcopy[m, s][1].wait_recv()
            hcopy[m, s][3].start()

    def out_cols(n):
        return pl.ds(pl.multiple_of(n * TILE, TILE), TILE)

    def to_inner(k, n):
        cols = out_cols(n)
        return remote(bp.at[k, :, cols], zs.at[k, :, cols], bp_s.at[k], zs_r.at[k, n], to_z[2])

    def to_owner(k, n):
        cols = out_cols(n)
        slot = k // 2
        return remote(bp.at[k, :, cols], zr.at[slot, :, cols], bp_s.at[k], bp_r.at[slot, n], to_z[k])

    def segments(t):
        (off_a, wid_a), (off_b, wid_b) = tiles[t]
        for who in range(2):
            yield who * na + off_a, wid_a
            yield base_b + who * nbw + off_b, wid_b

    def relays_in(m):
        for s in range(2):
            for i in (2, 3):
                hcopy[m, s][i].wait_recv()

    nn = width // TILE

    def s4(k, first, last):
        if first == 0:
            for t in range(nt):
                relays_in(k * nt + t)
        lhs = at(sets[k] * part, part, part)

        def body(n, carry):
            cols = out_cols(n)
            bp[k, :, cols] = jnp.dot(hid[lhs, :], wd[:, cols], preferred_element_type=F32).astype(BF16)
            if k == G - 2:
                to_owner(k, n).start()
            else:

                @pl.when(jnp.logical_not(inner))
                def _():
                    to_inner(k, n).start()

            return carry

        lax.fori_loop(first, last, body, 0)

    def join(k):
        @pl.when(inner)
        def _():
            def body(n, carry):
                cols = out_cols(n)
                to_inner(k, n).wait_recv()
                bp[k, :, cols] = (bp[k, :, cols].astype(F32) + zs[k, :, cols].astype(F32)).astype(BF16)
                to_owner(k, n).start()
                return carry

            lax.fori_loop(0, nn, body, 0)

    def s5(t):
        relays_in((G - 1) * nt + t)
        lhs = at(sets[G - 1] * part, part, part)
        late = t == nt - 1
        for n in range(nn):
            cols = pl.ds(n * TILE, TILE)
            acc = sum(
                jnp.dot(hid[lhs, lo : lo + w], wd[lo : lo + w, cols], preferred_element_type=F32)
                for lo, w in segments(t)
            )
            if t > 0:
                acc = acc + mix[:, cols]
            if late:
                for slot, k in ((0, 0), (1, 2)):
                    to_owner(k, n).wait_recv()
                    acc = acc + zr[slot, :, cols].astype(F32)
            if late:
                acc = acc * down_scale[:, cols]
                for i in range(2):
                    spot = at((i + y - 2 * i * y) * half, half, half)
                    mix[i * half : (i + 1) * half, cols] = (
                        0.5 * la[spot, cols].astype(F32) + acc[i * half : (i + 1) * half]
                    )
            else:
                mix[:, cols] = acc

    def weights_in(t):
        for s in range(2):
            wcopy[t, s].wait_recv()
            fcopy[t, s].start()

    def weights_ready(t):
        for s in range(2):
            fcopy[t, s].wait_recv()

    for i in range(PIECES - 1):
        arrive(1, i)
    weights_in(0)
    arrive(1, PIECES - 1)
    weights_ready(0)

    steps = G * nt
    for i in range(steps + SKEW[2]):
        if 0 < i < nt:
            weights_in(i)
            weights_ready(i)
        if i % nt == 0 and i < steps:
            if i // nt == G - 1:
                for j in range(PIECES):
                    arrive(G - 1, j)
            normalize(i // nt)
        if i < steps:
            s1(i)
        if 0 <= i - nt < PIECES // 2:
            arrive(2, 2 * (i - nt))
            arrive(2, 2 * (i - nt) + 1)
        if 0 <= i - SKEW[0] < steps:
            s2(i - SKEW[0])
        if 0 <= i - SKEW[1] < steps:
            s3(i - SKEW[1])
        m = i - SKEW[2]
        if m >= 0 and m % nt == nt - 1 and 0 < m // nt < G - 1:
            join(m // nt - 1)
        if 0 <= m < steps - nt and m % nt == nt - 1:
            s4(m // nt, 0, nn // 2 if m // nt < G - 2 else nn)
        if nt <= m < steps - nt and m % nt == 0:
            s4(m // nt - 1, nn // 2, nn)
        if steps - nt <= m < steps:
            s5(m - (steps - nt))

    put_stats(mix[...], st2, 0)
    swap2 = swap_stats(st2, 1)
    for copy in swap2:
        copy.start()
    for copy in swap1 + gains:
        copy.wait_send()
    for k in range(G - 1):
        remote(bp.at[k], bp.at[k], bp_s.at[k], bp_r.at[0, 0], to_x).wait_send()
    for j in range(2):
        ref = tok.at[pl.ds(0, part), :]
        remote(ref, ref, tok_s.at[j], tok_r.at[j, 0], to_x).wait_send()
    for s in range(2):
        mine, away = ((sa, ca), (sb, cb))[s]
        remote(mine, mine, w_s.at[s], w_r.at[0, s], to_x).wait_send()
        remote(mine, mine, f_s.at[s], f_r.at[0, s], to_x).wait_send()
        remote(away, away, c_s.at[s], c_r.at[s, 0], to_x).wait_send()
        for i in range(4):
            ref = away.at[0] if i < 2 else away.at[0, pl.ds(0, rows // 4)]
            remote(ref, ref, h_s.at[s, i], h_r.at[s, i, 0], to_x).wait_send()
    for way in range(2):
        for dist in range(G - 1):

            @pl.when(
                jnp.logical_and(r >= dist, r < G - 1)
                if way == 0
                else jnp.logical_and(r <= G - 1 - dist, r > 0)
            )
            def _():
                ref = xt.at[:, pl.ds(0, part), :]
                remote(ref, ref, z_s.at[way, dist], z_r.at[way, dist, 0, 0], to_x).wait_send()
    for copy in swap2:
        copy.wait_recv()
    both = get_stats(st2, 0, part)
    final = []
    for i in range(2):
        spot = pl.ds(i * half, half)
        mean, inv = both[i * half : (i + 1) * half, 0:1], both[i * half : (i + 1) * half, 1:2]
        out[spot, :] = ((mix[spot, :] - mean) * inv * og[...] + ob[...]).astype(BF16)
        final.append(pltpu.make_async_copy(out.at[spot, :], out_hbm.at[spot, :], out_sem.at[i]))
        final[i].start()

    for copy in swap2:
        copy.wait_send()
    for copy in final:
        copy.wait()


def fused(
    tokens,
    norm_gain,
    norm_bias,
    gate_weight,
    up_weight,
    gate_scale,
    up_scale,
    down_weight,
    down_scale,
    out_gain,
    out_bias,
):
    rows, width = tokens.shape
    ff = gate_weight.shape[1]
    na, nbw, tiles = tiles_of(ff)
    nt = len(tiles)
    part = rows // G
    half = part // 2
    kh = width // 2
    steps = G * nt
    hbm = pl.BlockSpec(memory_space=pl.ANY)
    row = lambda v: v.reshape(1, -1)
    dma = pltpu.SemaphoreType.DMA
    return pl.pallas_call(
        kernel,
        out_shape=jax.ShapeDtypeStruct((part, width), BF16),
        in_specs=[hbm] * 11,
        out_specs=hbm,
        scratch_shapes=[
            pltpu.VMEM((rows, width), BF16),
            pltpu.VMEM((1, width), F32),
            pltpu.VMEM((1, width), F32),
            pltpu.VMEM((ff // LANE, LANE), F32),
            pltpu.VMEM((ff // LANE, LANE), F32),
            pltpu.VMEM((1, width), F32),
            pltpu.VMEM((1, width), F32),
            pltpu.VMEM((1, width), F32),
            pltpu.VMEM((part, width), BF16),
            pltpu.VMEM((4, width, TILE), F32),
            pltpu.VMEM((2, TILE, width), F32),
            pltpu.VMEM((2, 2 * width, na), BF16),
            pltpu.VMEM((2, 2 * width, nbw), BF16),
            pltpu.VMEM((2, kh, na), BF16),
            pltpu.VMEM((2, kh, nbw), BF16),
            pltpu.VMEM((2, rows, width), BF16),
            pltpu.VMEM((2, 2, 1, width), F32),
            pltpu.VMEM((part, 2 * width), BF16),
            pltpu.VMEM((part, 2 * width), BF16),
            pltpu.VMEM((2, rows // 2, na), F32),
            pltpu.VMEM((2, rows // 2, nbw), F32),
            pltpu.VMEM((2, rows // 2, na), BF16),
            pltpu.VMEM((2, rows // 2, nbw), BF16),
            pltpu.VMEM((2, rows // 2, na), BF16),
            pltpu.VMEM((2, rows // 2, nbw), BF16),
            pltpu.VMEM((rows, ff), BF16),
            pltpu.VMEM((ff, width), BF16),
            pltpu.VMEM((G - 1, part, width), BF16),
            pltpu.VMEM((2, part, width), BF16),
            pltpu.VMEM((2, part, width), BF16),
            pltpu.VMEM((part, width), F32),
            pltpu.VMEM((rows, LANE), F32),
            pltpu.VMEM((G, 8, rows), F32),
            pltpu.VMEM((G, 8, part), F32),
            dma((G + 7,)),
            dma((2,)),
            dma((4, 2)),
            dma((2,)),
            dma((2,)),
            dma((2, PIECES)),
            dma((2, G - 1)),
            dma((2, G - 1, 2, PIECES)),
            dma((2, 2)),
            dma((2, 2)),
            dma((2,)),
            dma((nt, 2)),
            dma((2,)),
            dma((nt, 2)),
            dma((2,)),
            dma((2, steps)),
            dma((2, 4)),
            dma((2, 4, steps)),
            dma((G - 1,)),
            dma((2, width // TILE)),
            dma((2, width // TILE)),
            dma((2, G - 1)),
            dma((2, G - 1)),
        ],
        compiler_params=pltpu.CompilerParams(
            collective_id=0, has_side_effects=True, vmem_limit_bytes=67043328
        ),
    )(
        tokens,
        row(norm_gain),
        row(norm_bias),
        gate_weight,
        up_weight,
        gate_scale.reshape(-1, LANE),
        up_scale.reshape(-1, LANE),
        down_weight,
        row(down_scale),
        row(out_gain),
        row(out_bias),
    )


def local(*args):
    rows, width = args[0].shape
    ff = args[3].shape[1]
    fits = (
        lax.axis_size("cb") == G
        and lax.axis_size("ra") == G
        and lax.axis_size("dp") == 2
        and rows % (256 * G) == 0
        and width % TILE == 0
        and ff % TILE == 0
        and min(pair[1][1] for pair in tiles_of(ff)[2]) > 0
        and rows * width <= 1 << 20
        and ff * width <= 2816 * 1024
    )
    return (fused if fits else plain)(*args)


def solution(mesh):
    return jax.shard_map(
        local,
        mesh=mesh,
        in_specs=(
            P("dp", "cb"),
            P("cb"),
            P("cb"),
            P("cb", "ra"),
            P("cb", "ra"),
            P("ra"),
            P("ra"),
            P("ra", "cb"),
            P("cb"),
            P("cb"),
            P("cb"),
        ),
        out_specs=P(("dp", "ra"), "cb"),
        check_vma=False,
    )
```

```python
import jax
import jax.numpy as jnp
from jax import lax
from jax.experimental import pallas as pl
from jax.experimental.pallas import tpu as pltpu
from jax.sharding import PartitionSpec as P

MESH = pl.DeviceIdType.MESH
EPS = 1e-05
TILE = 256
LANE = 128
PIECES = 4
G = 4
F32 = jnp.float32
BF16 = jnp.bfloat16


def standardize(values):
    width = values.shape[1] * lax.axis_size("cb")
    total = lax.psum(jnp.sum(values, axis=1), "cb")
    mean = total / width
    centred = values - mean[:, None]
    spread = lax.psum(jnp.sum(centred * centred, axis=1), "cb") / width
    return centred * lax.rsqrt(spread + EPS)[:, None]


def plain(
    tokens,
    norm_gain,
    norm_bias,
    gate_weight,
    up_weight,
    gate_scale,
    up_scale,
    down_weight,
    down_scale,
    out_gain,
    out_bias,
):
    normed = (standardize(tokens.astype(F32)) * norm_gain + norm_bias).astype(BF16)
    gate_part = jnp.dot(normed, gate_weight.astype(BF16), preferred_element_type=F32)
    up_part = jnp.dot(normed, up_weight.astype(BF16), preferred_element_type=F32)
    gate_share, up_share = (
        lax.psum_scatter(part.astype(BF16), "cb", scatter_dimension=1, tiled=True).astype(F32)
        for part in (gate_part, up_part)
    )
    share = gate_share.shape[1]
    offset = lax.axis_index("cb") * share
    gate_cols = lax.dynamic_slice_in_dim(gate_scale, offset, share, 0)
    up_cols = lax.dynamic_slice_in_dim(up_scale, offset, share, 0)
    hidden_share = (jax.nn.silu(gate_share * gate_cols) * (up_share * up_cols)).astype(BF16)
    hidden = lax.all_gather(hidden_share, "cb", axis=1, tiled=True)
    own_rows = hidden.shape[0] // lax.axis_size("ra")
    part = jnp.dot(hidden, down_weight.astype(BF16), preferred_element_type=F32)
    branch = lax.psum_scatter(part, "ra", scatter_dimension=0, tiled=True) * down_scale
    own_normed = lax.dynamic_slice_in_dim(normed, lax.axis_index("ra") * own_rows, own_rows, 0)
    mixed = 0.5 * own_normed.astype(F32) + branch
    return (standardize(mixed) * out_gain + out_bias).astype(BF16)


def tiles_of(ff):
    wide = (ff // LANE + 3) // 4 * LANE
    narrow = ff // 2 - wide
    count = (wide + TILE - 1) // TILE
    both = []
    for t in range(count):
        off = t * TILE
        both.append(((off, min(TILE, wide - off)), (off, min(TILE, narrow - off))))
    return wide, narrow, both


def kernel(
    tok_hbm,
    ng_hbm,
    nb_hbm,
    gw,
    uw,
    gs_hbm,
    us_hbm,
    dw,
    ds_hbm,
    og_hbm,
    ob_hbm,
    out,
    tok,
    ng,
    nb,
    gs,
    us,
    down_scale,
    og,
    ob,
    stage,
    stage_d,
    wa,
    wb,
    sa,
    sb,
    xt,
    gb,
    la,
    lb,
    pa,
    pb,
    ca,
    cb,
    ra,
    rb,
    hid,
    wd,
    bp,
    zr,
    zs,
    mix,
    ms,
    st,
    st2,
    in_sem,
    stage_sem,
    stage_d_sem,
    tok_s,
    tok_r,
    z_s,
    z_r,
    gb_s,
    gb_r,
    w_s,
    w_r,
    f_s,
    f_r,
    c_s,
    c_r,
    h_s,
    h_r,
    bp_s,
    bp_r,
    zs_r,
    st_s,
    st_r,
):
    rows, width = tok.shape
    ff = gw.shape[1]
    na, nbw, tiles = tiles_of(ff)
    nt = len(tiles)
    base_b = 2 * na
    part = rows // G
    half = part // 2
    piece = part // PIECES
    kh = width // 2
    full = float(width * G)

    b = lax.axis_index("cb")
    r = lax.axis_index("ra")
    p = lax.axis_index("dp")
    x = lax.rem(b, 2)
    y = b // 2
    to_x = {"cb": b + 1 - 2 * x}
    to_y = {"cb": b + 2 - 4 * y}
    to_d = {"cb": (G - 1) - b}
    twin = {"dp": 1 - p}
    hi = r // 2
    sets = [3 - 3 * hi, 2 - hi, r + 1 - 2 * lax.rem(r, 2), r]
    inner = lax.rem(r, 2) + hi == 1
    to_z = [{"ra": s} for s in sets[:3]]
    ring = [{"ra": lax.rem(r + o, G)} for o in range(1, G)]

    barrier = pltpu.get_barrier_semaphore()
    greet = [to_x, to_y, to_d, twin] + ring
    for peer in greet:
        pl.semaphore_signal(barrier, inc=1, device_id=peer, device_id_type=MESH)

    small = [
        pltpu.make_async_copy(src, dst, in_sem.at[G + i])
        for i, (src, dst) in enumerate(
            (
                (ng_hbm, ng),
                (nb_hbm, nb),
                (gs_hbm, gs),
                (us_hbm, us),
                (ds_hbm, down_scale),
                (og_hbm, og),
                (ob_hbm, ob),
            )
        )
    ]
    tok_in = [
        pltpu.make_async_copy(
            tok_hbm.at[pl.ds(pl.multiple_of(q * part, part), part), :],
            tok.at[pl.ds(pl.multiple_of(q * part, part), part), :],
            in_sem.at[j],
        )
        for j, q in enumerate(lax.rem(G - 1 - r + j, G) for j in range(G))
    ]
    for copy in tok_in + small:
        copy.start()

    def at(start, size, align):
        return pl.ds(pl.multiple_of(start, align), size)

    def remote(src, dst, send, recv, peer):
        return pltpu.make_async_remote_copy(
            src_ref=src,
            dst_ref=dst,
            send_sem=send,
            recv_sem=recv,
            device_id=peer,
            device_id_type=MESH,
        )

    def a_cols(t, who):
        off, w = tiles[t][0]
        return at(who * na + off, w, LANE)

    def b_cols(t, who):
        off, w = tiles[t][1]
        return at(base_b + who * nbw + off, w, LANE)

    def load_send(kind, t):
        slot = t % 2
        src = (gw, uw)[kind % 2]
        cols = a_cols(t, 1 - x) if kind < 2 else b_cols(t, 1 - y)
        w = tiles[t][kind // 2][1]
        return pltpu.make_async_copy(
            src.at[at(p * kh, kh, kh), cols],
            stage.at[kind, pl.ds(slot * kh, kh), pl.ds(0, w)],
            stage_sem.at[kind, slot],
        )

    def load_own(kind, t):
        src = (gw, uw)[kind % 2]
        cols = a_cols(t, x) if kind < 2 else b_cols(t, y)
        w = tiles[t][kind // 2][1]
        return pltpu.make_async_copy(
            src.at[:, cols], stage.at[kind, :, pl.ds(0, w)], stage_sem.at[kind, 0]
        )

    def tile_rows(t):
        return pl.ds(pl.multiple_of(t * TILE, TILE), TILE)

    def load_d(t, slot):
        return pltpu.make_async_copy(dw.at[tile_rows(t), :], stage_d.at[slot], stage_d_sem.at[slot])

    for t in range(min(2, nt)):
        for kind in range(4):
            load_send(kind, t).start()
    for t in range(2):
        load_d(t, t).start()

    tok_in[0].wait()
    pl.semaphore_wait(barrier, len(greet))

    own_tok = []
    for i in range(PIECES):
        rows_i = at((G - 1 - r) * part + i * piece, piece, piece)
        for j, peer in enumerate((to_x, to_y)):
            own_tok.append(
                remote(tok.at[rows_i, :], xt.at[j, rows_i, :], tok_s.at[j], tok_r.at[j, i], peer)
            )
    for copy in own_tok:
        copy.start()
    for copy in tok_in[1:] + small:
        copy.wait()

    def put_stats(v, dst, col):
        total = jnp.sum(v, axis=1, keepdims=True)
        off = v - total * (1.0 / width)
        spread = jnp.sum(off * off, axis=1, keepdims=True)
        lane = lax.broadcasted_iota(jnp.int32, (v.shape[0], LANE), 1)
        both = jnp.where(lane == 0, total, spread)
        dst[0, :, pl.ds(col, v.shape[0])] = both.T[:8, :]

    def get_stats(src, col, n):
        parts = [src[i, 0:2, pl.ds(col, n)] for i in range(G)]
        mean = (parts[0][0:1] + parts[1][0:1] + parts[2][0:1] + parts[3][0:1]) / full
        spread = jnp.zeros_like(mean)
        for q in parts:
            d = q[0:1] * (1.0 / width) - mean
            spread = spread + q[1:2] + width * (d * d)
        inv = lax.rsqrt(spread / full + EPS)
        sub = lax.broadcasted_iota(jnp.int32, (LANE, n), 0)
        return jnp.where(sub == 0, mean, inv).T

    def swap_stats(buf, which):
        return [
            remote(buf.at[0, pl.ds(0, 2)], buf.at[1 + i, pl.ds(0, 2)], st_s.at[which, i], st_r.at[which, i], peer)
            for i, peer in enumerate((to_x, to_y, to_d))
        ]

    for j in range(G):
        put_stats(tok[pl.ds(j * part, part), :].astype(F32), st, j * part)
    swap1 = swap_stats(st, 0)
    for copy in swap1:
        copy.start()
    gains = []
    for j, peer in enumerate((to_x, to_y)):
        for i, ref in enumerate((ng, nb)):
            gains.append(remote(ref, gb.at[j, i], gb_s.at[j, i], gb_r.at[j, i], peer))
    for copy in gains:
        copy.start()

    wcopy = {}
    fcopy = {}
    for t in range(nt):
        for s in range(2):
            off, w = tiles[t][s]
            mine = (sa, sb)[s].at[:, :, pl.ds(off, w)]
            there = (wa, wb)[s].at[:, at(width + p * kh, kh, kh), pl.ds(off, w)]
            wcopy[t, s] = remote(mine, there, w_s.at[s], w_r.at[t, s], (to_x, to_y)[s])
            fcopy[t, s] = remote(there, there, f_s.at[s], f_r.at[t, s], twin)

    def send_weights(t):
        for kind in range(4):
            load_send(kind, t).wait()
            s, g = kind // 2, kind % 2
            off, w = tiles[t][s]
            (sa, sb)[s][g, :, off : off + w] = stage[kind, (t % 2) * kh : (t % 2 + 1) * kh, 0:w].astype(BF16)
            if t + 2 < nt:
                load_send(kind, t + 2).start()
        for s in range(2):
            wcopy[t, s].start()

    def zcopy(way, dist, j, i):
        q = r - dist if way == 0 else r + dist
        rows_q = at((G - 1 - q) * part + i * piece, piece, piece)
        ref = xt.at[j, rows_q, :]
        peer = {"ra": r + 1 if way == 0 else r - 1}
        return remote(ref, ref, z_s.at[way, dist], z_r.at[way, dist, j, i], peer)

    def spread_own(i):
        for j in range(2):
            own_tok[2 * i + j].wait_recv()
        for way in range(2):

            @pl.when((r < G - 1) if way == 0 else (r > 0))
            def _():
                for j in range(2):
                    zcopy(way, 0, j, i).start()

    def arrive(dist, i):
        for way in range(2):

            @pl.when((r >= dist) if way == 0 else (r <= G - 1 - dist))
            def _():
                q = r - dist if way == 0 else r + dist
                rows_q = at((G - 1 - q) * part + i * piece, piece, piece)
                for j in range(2):
                    ref = xt.at[j, rows_q, :]
                    remote(
                        ref, ref, z_s.at[way, dist - 1], z_r.at[way, dist - 1, j, i], to_x
                    ).wait_recv()

            if dist < G - 1:

                @pl.when(
                    jnp.logical_and(r >= dist, r < G - 1)
                    if way == 0
                    else jnp.logical_and(r <= G - 1 - dist, r > 0)
                )
                def _():
                    for j in range(2):
                        zcopy(way, dist, j, i).start()

    for t in range(nt):
        send_weights(t)
    for kind in range(4):
        load_own(kind, 0).start()

    spread_own(0)
    spread_own(1)
    for t in range(nt):
        for kind in range(4):
            load_own(kind, t).wait()
            s, g = kind // 2, kind % 2
            off, w = tiles[t][s]
            (wa, wb)[s][g, 0:width, off : off + w] = stage[kind, :, 0:w].astype(BF16)
            if t + 1 < nt:
                load_own(kind, t + 1).start()
    spread_own(2)
    for copy in swap1:
        copy.wait_recv()
    for j in range(G):
        ms[pl.ds(j * part, part), :] = get_stats(st, j * part, part)
    spread_own(3)
    for copy in gains:
        copy.wait_recv()

    def cast_d(t, carry):
        slot = lax.rem(t, 2)
        load_d(t, slot).wait()
        wd[tile_rows(t), :] = stage_d[slot].astype(BF16)

        @pl.when(t + 2 < ff // TILE)
        def _():
            load_d(t + 2, slot).start()

        return carry

    lax.fori_loop(0, ff // TILE, cast_d, 0)

    def normalize(k):
        slot = k % 2
        for i in range(2):
            rows_i = at(sets[k] * part + i * half, half, half)
            both = ms[rows_i, :]
            mean, inv = both[:, 0:1], both[:, 1:2]

            def norm(v, gain, bias):
                return ((v.astype(F32) - mean) * inv * gain + bias).astype(BF16)

            for lhs, j, side in ((la, 0, y), (lb, 1, x)):
                spot = at((i + side - 2 * i * side) * half, half, half)
                lhs[slot, spot, 0:width] = norm(tok[rows_i, :], ng[...], nb[...])
                lhs[slot, spot, width : 2 * width] = norm(xt[j, rows_i, :], gb[j, 0], gb[j, 1])

    ccopy = {}
    hcopy = {}
    for k in range(G):
        for t in range(nt):
            m = k * nt + t
            spot = pl.ds(k * half, half)
            for s in range(2):
                off, w = tiles[t][s]
                region = (ca, cb)[s].at[:, spot, pl.ds(off, w)]
                land = (ra, rb)[s].at[:, spot, pl.ds(off, w)]
                ccopy[m, s] = remote(region, land, c_s.at[s], c_r.at[s, m], (to_y, to_x)[s])
                side, who = ((y, x), (x, y))[s]
                cols = (a_cols, b_cols)[s]

                def block(side_, who_, lo, n):
                    return hid.at[at(sets[k] * part + side_ * half + lo, n, n), cols(t, who_)]

                own = block(side, who, 0, half)
                of_x = block(side, 1 - who, 0, half // 2) if s == 0 else block(1 - side, who, 0, half // 2)
                of_y = (
                    block(1 - side, who, half // 2, half // 2)
                    if s == 0
                    else block(side, 1 - who, half // 2, half // 2)
                )
                hcopy[m, s] = [
                    remote(own, own, h_s.at[s, 0], h_r.at[s, 0, m], to_x),
                    remote(own, own, h_s.at[s, 1], h_r.at[s, 1, m], to_y),
                    remote(of_x, of_x, h_s.at[s, 2], h_r.at[s, 2, m], to_y),
                    remote(of_y, of_y, h_s.at[s, 3], h_r.at[s, 3, m], to_x),
                ]

    def scale_row(ref, s, t, who):
        off, w = tiles[t][s]
        first = (s * base_b + who * (na, nbw)[s] + off) // LANE
        return jnp.concatenate([ref[pl.ds(first + i, 1), :] for i in range(w // LANE)], axis=1)

    def s1(m):
        k, t = m // nt, m % nt
        for s in range(2):
            off, w = tiles[t][s]
            lhs, wgt, keep, away = ((la, wa, pa, ca), (lb, wb, pb, cb))[s]

            def one(g, carry):
                acc = jnp.dot(lhs[k % 2], wgt[g, :, off : off + w], preferred_element_type=F32)
                keep[g, k * half : (k + 1) * half, off : off + w] = acc[:half]
                away[g, k * half : (k + 1) * half, off : off + w] = acc[half:].astype(BF16)
                return carry

            lax.fori_loop(0, 2, one, 0)
            ccopy[m, s].start()

    def s2(m, sides=(0, 1)):
        k, t = m // nt, m % nt
        for s in sides:
            ccopy[m, s].wait_recv()
            off, w = tiles[t][s]
            keep, got = ((pa, ra), (pb, rb))[s]
            side, who = ((y, x), (x, y))[s]
            cols = (a_cols, b_cols)[s](t, who)
            spot = pl.ds(k * half, half)
            g = keep[0, spot, off : off + w] + got[0, spot, off : off + w].astype(F32)
            u = keep[1, spot, off : off + w] + got[1, spot, off : off + w].astype(F32)
            g = g * scale_row(gs, s, t, who)
            u = u * scale_row(us, s, t, who)
            h = (g / (1.0 + jnp.exp(-g)) * u).astype(BF16)
            hid[at(sets[k] * part + side * half, half, half), cols] = h
            hcopy[m, s][0].start()
            hcopy[m, s][1].start()

    def s3(m):
        for s in range(2):
            hcopy[m, s][0].wait_recv()
            hcopy[m, s][2].start()
            hcopy[m, s][1].wait_recv()
            hcopy[m, s][3].start()

    def out_cols(n):
        return pl.ds(pl.multiple_of(n * TILE, TILE), TILE)

    def to_inner(k, n):
        cols = out_cols(n)
        return remote(bp.at[k, :, cols], zs.at[k, :, cols], bp_s.at[k], zs_r.at[k, n], to_z[2])

    def to_owner(k, n):
        cols = out_cols(n)
        slot = k // 2
        return remote(bp.at[k, :, cols], zr.at[slot, :, cols], bp_s.at[k], bp_r.at[slot, n], to_z[k])

    def segments(t):
        (off_a, wid_a), (off_b, wid_b) = tiles[t]
        for who in range(2):
            yield who * na + off_a, wid_a
            yield base_b + who * nbw + off_b, wid_b

    def relays_in(m):
        for s in range(2):
            for i in (2, 3):
                hcopy[m, s][i].wait_recv()

    nn = width // TILE

    def s4(k, first, last):
        if first == 0:
            for t in range(nt):
                relays_in(k * nt + t)
        lhs = at(sets[k] * part, part, part)

        def body(n, carry):
            cols = out_cols(n)
            bp[k, :, cols] = jnp.dot(hid[lhs, :], wd[:, cols], preferred_element_type=F32).astype(BF16)
            if k == G - 2:
                to_owner(k, n).start()
            else:

                @pl.when(jnp.logical_not(inner))
                def _():
                    to_inner(k, n).start()

            return carry

        lax.fori_loop(first, last, body, 0)

    def join(k):
        @pl.when(inner)
        def _():
            def body(n, carry):
                cols = out_cols(n)
                to_inner(k, n).wait_recv()
                bp[k, :, cols] = (bp[k, :, cols].astype(F32) + zs[k, :, cols].astype(F32)).astype(BF16)
                to_owner(k, n).start()
                return carry

            lax.fori_loop(0, nn, body, 0)

    def s5(t):
        relays_in((G - 1) * nt + t)
        lhs = at(sets[G - 1] * part, part, part)
        late = t == nt - 1
        for n in range(nn):
            cols = pl.ds(n * TILE, TILE)
            acc = sum(
                jnp.dot(hid[lhs, lo : lo + w], wd[lo : lo + w, cols], preferred_element_type=F32)
                for lo, w in segments(t)
            )
            if t > 0:
                acc = acc + mix[:, cols]
            if late:
                for slot, k in ((0, 0), (1, 2)):
                    to_owner(k, n).wait_recv()
                    acc = acc + zr[slot, :, cols].astype(F32)
            if late:
                acc = acc * down_scale[:, cols]
                for i in range(2):
                    spot = at((i + y - 2 * i * y) * half, half, half)
                    mix[i * half : (i + 1) * half, cols] = (
                        0.5 * la[(G - 1) % 2, spot, cols].astype(F32) + acc[i * half : (i + 1) * half]
                    )
            else:
                mix[:, cols] = acc

    def weights_in(t):
        for s in range(2):
            wcopy[t, s].wait_recv()
            fcopy[t, s].start()

    def weights_ready(t):
        for s in range(2):
            fcopy[t, s].wait_recv()

    steps = G * nt
    first = 2 * nt

    for i in range(PIECES - 1):
        arrive(1, i)
    weights_in(0)
    arrive(1, PIECES - 1)
    normalize(0)
    normalize(1)
    weights_ready(0)
    s1(0)
    s1(nt)
    for t in range(1, nt):
        if t == nt - 1:
            s2(0, (0,))
        weights_in(t)
        weights_ready(t)
        s1(t)
        if t == nt - 1:
            s2(0, (1,))
        s1(nt + t)
        for j in range(PIECES):
            if 1 + j * (nt - 1) // PIECES == t:
                arrive(2, j)
    for i in range(2, first):
        if i == first - 1:
            normalize(2)
            s1(first)
        s2(i - 1)
        s3(i - 2)
    s4(0, 0, nn)

    for i in range(first, steps + 3):
        if i < steps and i > first:
            if i == steps - nt:
                for j in range(PIECES):
                    arrive(G - 1, j)
                normalize(G - 1)
            s1(i)
        k = i // nt - 1
        edge = i % nt == nt - 1 and k < G - 1
        early = i == steps - nt + 1
        if early:
            s3(i - 2)
        if i - 1 < steps:
            s2(i - 1)
        if edge and k == 2:
            join(1)
            s4(2, 0, nn)
        if not early and i - 2 < steps:
            s3(i - 2)
        if edge:
            if k < 2:
                s4(k, 0, nn)
            if k == 1:
                join(0)
        if i >= steps and i - steps < nt:
            s5(i - steps)

    put_stats(mix[...], st2, 0)
    swap2 = swap_stats(st2, 1)
    for copy in swap2:
        copy.start()
    for copy in swap1 + gains:
        copy.wait_send()
    for k in range(G - 1):
        remote(bp.at[k], bp.at[k], bp_s.at[k], bp_r.at[0, 0], to_x).wait_send()
    for j in range(2):
        ref = tok.at[pl.ds(0, part), :]
        remote(ref, ref, tok_s.at[j], tok_r.at[j, 0], to_x).wait_send()
    for s in range(2):
        mine, away = ((sa, ca), (sb, cb))[s]
        remote(mine, mine, w_s.at[s], w_r.at[0, s], to_x).wait_send()
        remote(mine, mine, f_s.at[s], f_r.at[0, s], to_x).wait_send()
        remote(away, away, c_s.at[s], c_r.at[s, 0], to_x).wait_send()
        for i in range(4):
            ref = away.at[0] if i < 2 else away.at[0, pl.ds(0, rows // 4)]
            remote(ref, ref, h_s.at[s, i], h_r.at[s, i, 0], to_x).wait_send()
    for way in range(2):
        for dist in range(G - 1):

            @pl.when(
                jnp.logical_and(r >= dist, r < G - 1)
                if way == 0
                else jnp.logical_and(r <= G - 1 - dist, r > 0)
            )
            def _():
                ref = xt.at[:, pl.ds(0, part), :]
                remote(ref, ref, z_s.at[way, dist], z_r.at[way, dist, 0, 0], to_x).wait_send()
    for copy in swap2:
        copy.wait_recv()
    both = get_stats(st2, 0, part)
    for i in range(2):
        spot = pl.ds(i * half, half)
        mean, inv = both[i * half : (i + 1) * half, 0:1], both[i * half : (i + 1) * half, 1:2]
        out[spot, :] = ((mix[spot, :] - mean) * inv * og[...] + ob[...]).astype(BF16)

    for copy in swap2:
        copy.wait_send()


def fused(
    tokens,
    norm_gain,
    norm_bias,
    gate_weight,
    up_weight,
    gate_scale,
    up_scale,
    down_weight,
    down_scale,
    out_gain,
    out_bias,
):
    rows, width = tokens.shape
    ff = gate_weight.shape[1]
    na, nbw, tiles = tiles_of(ff)
    nt = len(tiles)
    part = rows // G
    half = part // 2
    kh = width // 2
    steps = G * nt
    hbm = pl.BlockSpec(memory_space=pl.ANY)
    row = lambda v: v.reshape(1, -1)
    dma = pltpu.SemaphoreType.DMA
    return pl.pallas_call(
        kernel,
        out_shape=pltpu.VMEM((part, width), BF16),
        in_specs=[hbm] * 11,
        out_specs=pl.BlockSpec(memory_space=pltpu.VMEM),
        scratch_shapes=[
            pltpu.VMEM((rows, width), BF16),
            pltpu.VMEM((1, width), F32),
            pltpu.VMEM((1, width), F32),
            pltpu.VMEM((ff // LANE, LANE), F32),
            pltpu.VMEM((ff // LANE, LANE), F32),
            pltpu.VMEM((1, width), F32),
            pltpu.VMEM((1, width), F32),
            pltpu.VMEM((1, width), F32),
            pltpu.VMEM((4, width, TILE), F32),
            pltpu.VMEM((2, TILE, width), F32),
            pltpu.VMEM((2, 2 * width, na), BF16),
            pltpu.VMEM((2, 2 * width, nbw), BF16),
            pltpu.VMEM((2, kh, na), BF16),
            pltpu.VMEM((2, kh, nbw), BF16),
            pltpu.VMEM((2, rows, width), BF16),
            pltpu.VMEM((2, 2, 1, width), F32),
            pltpu.VMEM((2, part, 2 * width), BF16),
            pltpu.VMEM((2, part, 2 * width), BF16),
            pltpu.VMEM((2, rows // 2, na), F32),
            pltpu.VMEM((2, rows // 2, nbw), F32),
            pltpu.VMEM((2, rows // 2, na), BF16),
            pltpu.VMEM((2, rows // 2, nbw), BF16),
            pltpu.VMEM((2, rows // 2, na), BF16),
            pltpu.VMEM((2, rows // 2, nbw), BF16),
            pltpu.VMEM((rows, ff), BF16),
            pltpu.VMEM((ff, width), BF16),
            pltpu.VMEM((G - 1, part, width), BF16),
            pltpu.VMEM((2, part, width), BF16),
            pltpu.VMEM((2, part, width), BF16),
            pltpu.VMEM((part, width), F32),
            pltpu.VMEM((rows, LANE), F32),
            pltpu.VMEM((G, 8, rows), F32),
            pltpu.VMEM((G, 8, part), F32),
            dma((G + 7,)),
            dma((4, 2)),
            dma((2,)),
            dma((2,)),
            dma((2, PIECES)),
            dma((2, G - 1)),
            dma((2, G - 1, 2, PIECES)),
            dma((2, 2)),
            dma((2, 2)),
            dma((2,)),
            dma((nt, 2)),
            dma((2,)),
            dma((nt, 2)),
            dma((2,)),
            dma((2, steps)),
            dma((2, 4)),
            dma((2, 4, steps)),
            dma((G - 1,)),
            dma((2, width // TILE)),
            dma((2, width // TILE)),
            dma((2, G - 1)),
            dma((2, G - 1)),
        ],
        compiler_params=pltpu.CompilerParams(
            collective_id=0, has_side_effects=True, vmem_limit_bytes=63500000
        ),
    )(
        tokens,
        row(norm_gain),
        row(norm_bias),
        gate_weight,
        up_weight,
        gate_scale.reshape(-1, LANE),
        up_scale.reshape(-1, LANE),
        down_weight,
        row(down_scale),
        row(out_gain),
        row(out_bias),
    )


def local(*args):
    rows, width = args[0].shape
    ff = args[3].shape[1]
    fits = (
        lax.axis_size("cb") == G
        and lax.axis_size("ra") == G
        and lax.axis_size("dp") == 2
        and rows % (256 * G) == 0
        and width % TILE == 0
        and ff % TILE == 0
        and min(pair[1][1] for pair in tiles_of(ff)[2]) > 0
        and rows * width <= 1 << 20
        and ff * width <= 2816 * 1024
    )
    return (fused if fits else plain)(*args)


def solution(mesh):
    return jax.shard_map(
        local,
        mesh=mesh,
        in_specs=(
            P("dp", "cb"),
            P("cb"),
            P("cb"),
            P("cb", "ra"),
            P("cb", "ra"),
            P("ra"),
            P("ra"),
            P("ra", "cb"),
            P("cb"),
            P("cb"),
            P("cb"),
        ),
        out_specs=P(("dp", "ra"), "cb"),
        check_vma=False,
    )
```

```python
import jax
import jax.numpy as jnp
from jax import lax
from jax.experimental import pallas as pl
from jax.experimental.pallas import tpu as pltpu
from jax.sharding import PartitionSpec as P

MESH = pl.DeviceIdType.MESH
EPS = 1e-05
TILE = 256
LANE = 128
PIECES = 4
G = 4
F32 = jnp.float32
BF16 = jnp.bfloat16


def standardize(values):
    width = values.shape[1] * lax.axis_size("cb")
    total = lax.psum(jnp.sum(values, axis=1), "cb")
    mean = total / width
    centred = values - mean[:, None]
    spread = lax.psum(jnp.sum(centred * centred, axis=1), "cb") / width
    return centred * lax.rsqrt(spread + EPS)[:, None]


def plain(
    tokens,
    norm_gain,
    norm_bias,
    gate_weight,
    up_weight,
    gate_scale,
    up_scale,
    down_weight,
    down_scale,
    out_gain,
    out_bias,
):
    normed = (standardize(tokens.astype(F32)) * norm_gain + norm_bias).astype(BF16)
    gate_part = jnp.dot(normed, gate_weight.astype(BF16), preferred_element_type=F32)
    up_part = jnp.dot(normed, up_weight.astype(BF16), preferred_element_type=F32)
    gate_share, up_share = (
        lax.psum_scatter(part.astype(BF16), "cb", scatter_dimension=1, tiled=True).astype(F32)
        for part in (gate_part, up_part)
    )
    share = gate_share.shape[1]
    offset = lax.axis_index("cb") * share
    gate_cols = lax.dynamic_slice_in_dim(gate_scale, offset, share, 0)
    up_cols = lax.dynamic_slice_in_dim(up_scale, offset, share, 0)
    hidden_share = (jax.nn.silu(gate_share * gate_cols) * (up_share * up_cols)).astype(BF16)
    hidden = lax.all_gather(hidden_share, "cb", axis=1, tiled=True)
    own_rows = hidden.shape[0] // lax.axis_size("ra")
    part = jnp.dot(hidden, down_weight.astype(BF16), preferred_element_type=F32)
    branch = lax.psum_scatter(part, "ra", scatter_dimension=0, tiled=True) * down_scale
    own_normed = lax.dynamic_slice_in_dim(normed, lax.axis_index("ra") * own_rows, own_rows, 0)
    mixed = 0.5 * own_normed.astype(F32) + branch
    return (standardize(mixed) * out_gain + out_bias).astype(BF16)


def tiles_of(ff):
    wide = (ff // LANE + 3) // 4 * LANE
    narrow = ff // 2 - wide
    count = (wide + TILE - 1) // TILE
    both = []
    for t in range(count):
        off = t * TILE
        both.append(((off, min(TILE, wide - off)), (off, min(TILE, narrow - off))))
    return wide, narrow, both


def kernel(
    tok_hbm,
    ng_hbm,
    nb_hbm,
    gw,
    uw,
    gs_hbm,
    us_hbm,
    dw,
    ds_hbm,
    og_hbm,
    ob_hbm,
    out,
    tok,
    ng,
    nb,
    gs,
    us,
    down_scale,
    og,
    ob,
    stage,
    stage_d,
    wa,
    wb,
    sa,
    sb,
    xt,
    gb,
    la,
    lb,
    pa,
    pb,
    ca,
    cb,
    ra,
    rb,
    hid,
    wd,
    bp,
    zr,
    zs,
    mix,
    ms,
    st,
    st2,
    in_sem,
    stage_sem,
    stage_d_sem,
    tok_s,
    tok_r,
    z_s,
    z_r,
    gb_s,
    gb_r,
    w_s,
    w_r,
    f_s,
    f_r,
    c_s,
    c_r,
    h_s,
    h_r,
    bp_s,
    bp_r,
    zs_r,
    st_s,
    st_r,
):
    rows, width = tok.shape
    ff = gw.shape[1]
    na, nbw, tiles = tiles_of(ff)
    nt = len(tiles)
    base_b = 2 * na
    part = rows // G
    half = part // 2
    piece = part // PIECES
    kh = width // 2
    full = float(width * G)

    b = lax.axis_index("cb")
    r = lax.axis_index("ra")
    p = lax.axis_index("dp")
    x = lax.rem(b, 2)
    y = b // 2
    to_x = {"cb": b + 1 - 2 * x}
    to_y = {"cb": b + 2 - 4 * y}
    to_d = {"cb": (G - 1) - b}
    twin = {"dp": 1 - p}
    hi = r // 2
    sets = [3 - 3 * hi, 2 - hi, r + 1 - 2 * lax.rem(r, 2), r]
    inner = lax.rem(r, 2) + hi == 1
    to_z = [{"ra": s} for s in sets[:3]]
    ring = [{"ra": lax.rem(r + o, G)} for o in range(1, G)]

    barrier = pltpu.get_barrier_semaphore()
    greet = [to_x, to_y, to_d, twin] + ring
    for peer in greet:
        pl.semaphore_signal(barrier, inc=1, device_id=peer, device_id_type=MESH)

    small = [
        pltpu.make_async_copy(src, dst, in_sem.at[G + i])
        for i, (src, dst) in enumerate(
            (
                (ng_hbm, ng),
                (nb_hbm, nb),
                (gs_hbm, gs),
                (us_hbm, us),
                (ds_hbm, down_scale),
                (og_hbm, og),
                (ob_hbm, ob),
            )
        )
    ]
    tok_in = [
        pltpu.make_async_copy(
            tok_hbm.at[pl.ds(pl.multiple_of(q * part, part), part), :],
            tok.at[pl.ds(pl.multiple_of(q * part, part), part), :],
            in_sem.at[j],
        )
        for j, q in enumerate(lax.rem(G - 1 - r + j, G) for j in range(G))
    ]
    for copy in tok_in + small:
        copy.start()

    def at(start, size, align):
        return pl.ds(pl.multiple_of(start, align), size)

    def remote(src, dst, send, recv, peer):
        return pltpu.make_async_remote_copy(
            src_ref=src,
            dst_ref=dst,
            send_sem=send,
            recv_sem=recv,
            device_id=peer,
            device_id_type=MESH,
        )

    def a_cols(t, who):
        off, w = tiles[t][0]
        return at(who * na + off, w, LANE)

    def b_cols(t, who):
        off, w = tiles[t][1]
        return at(base_b + who * nbw + off, w, LANE)

    def load_send(kind, t):
        slot = t % 2
        src = (gw, uw)[kind % 2]
        cols = a_cols(t, 1 - x) if kind < 2 else b_cols(t, 1 - y)
        w = tiles[t][kind // 2][1]
        return pltpu.make_async_copy(
            src.at[at(p * kh, kh, kh), cols],
            stage.at[kind, pl.ds(slot * kh, kh), pl.ds(0, w)],
            stage_sem.at[kind, slot],
        )

    def load_own(kind, t):
        src = (gw, uw)[kind % 2]
        cols = a_cols(t, x) if kind < 2 else b_cols(t, y)
        w = tiles[t][kind // 2][1]
        return pltpu.make_async_copy(
            src.at[:, cols], stage.at[kind, :, pl.ds(0, w)], stage_sem.at[kind, 0]
        )

    def tile_rows(t):
        return pl.ds(pl.multiple_of(t * TILE, TILE), TILE)

    def load_d(t, slot):
        return pltpu.make_async_copy(dw.at[tile_rows(t), :], stage_d.at[slot], stage_d_sem.at[slot])

    for t in range(min(2, nt)):
        for kind in range(4):
            load_send(kind, t).start()
    for t in range(2):
        load_d(t, t).start()

    tok_in[0].wait()
    pl.semaphore_wait(barrier, len(greet))

    own_tok = []
    for i in range(PIECES):
        rows_i = at((G - 1 - r) * part + i * piece, piece, piece)
        for j, peer in enumerate((to_x, to_y)):
            own_tok.append(
                remote(tok.at[rows_i, :], xt.at[j, rows_i, :], tok_s.at[j], tok_r.at[j, i], peer)
            )
    for copy in own_tok:
        copy.start()
    for copy in tok_in[1:] + small:
        copy.wait()

    def put_stats(v, dst, col):
        total = jnp.sum(v, axis=1, keepdims=True)
        off = v - total * (1.0 / width)
        spread = jnp.sum(off * off, axis=1, keepdims=True)
        lane = lax.broadcasted_iota(jnp.int32, (v.shape[0], LANE), 1)
        both = jnp.where(lane == 0, total, spread)
        dst[0, :, pl.ds(col, v.shape[0])] = both.T[:8, :]

    def get_stats(src, col, n):
        parts = [src[i, 0:2, pl.ds(col, n)] for i in range(G)]
        mean = (parts[0][0:1] + parts[1][0:1] + parts[2][0:1] + parts[3][0:1]) / full
        spread = jnp.zeros_like(mean)
        for q in parts:
            d = q[0:1] * (1.0 / width) - mean
            spread = spread + q[1:2] + width * (d * d)
        inv = lax.rsqrt(spread / full + EPS)
        sub = lax.broadcasted_iota(jnp.int32, (LANE, n), 0)
        return jnp.where(sub == 0, mean, inv).T

    def swap_stats(buf, which):
        return [
            remote(buf.at[0, pl.ds(0, 2)], buf.at[1 + i, pl.ds(0, 2)], st_s.at[which, i], st_r.at[which, i], peer)
            for i, peer in enumerate((to_x, to_y, to_d))
        ]

    for j in range(G):
        put_stats(tok[pl.ds(j * part, part), :].astype(F32), st, j * part)
    swap1 = swap_stats(st, 0)
    for copy in swap1:
        copy.start()
    gains = []
    for j, peer in enumerate((to_x, to_y)):
        for i, ref in enumerate((ng, nb)):
            gains.append(remote(ref, gb.at[j, i], gb_s.at[j, i], gb_r.at[j, i], peer))
    for copy in gains:
        copy.start()

    wcopy = {}
    fcopy = {}
    for t in range(nt):
        for s in range(2):
            off, w = tiles[t][s]
            mine = (sa, sb)[s].at[:, :, pl.ds(off, w)]
            there = (wa, wb)[s].at[:, at(width + p * kh, kh, kh), pl.ds(off, w)]
            wcopy[t, s] = remote(mine, there, w_s.at[s], w_r.at[t, s], (to_x, to_y)[s])
            fcopy[t, s] = remote(there, there, f_s.at[s], f_r.at[t, s], twin)

    def send_weights(t):
        for kind in range(4):
            load_send(kind, t).wait()
            s, g = kind // 2, kind % 2
            off, w = tiles[t][s]
            (sa, sb)[s][g, :, off : off + w] = stage[kind, (t % 2) * kh : (t % 2 + 1) * kh, 0:w].astype(BF16)
            if t + 2 < nt:
                load_send(kind, t + 2).start()
        for s in range(2):
            wcopy[t, s].start()

    def zcopy(way, dist, j, i):
        q = r - dist if way == 0 else r + dist
        rows_q = at((G - 1 - q) * part + i * piece, piece, piece)
        ref = xt.at[j, rows_q, :]
        peer = {"ra": r + 1 if way == 0 else r - 1}
        return remote(ref, ref, z_s.at[way, dist], z_r.at[way, dist, i], peer)

    def spread_own(i):
        for j in range(2):
            own_tok[2 * i + j].wait_recv()
        for way in range(2):

            @pl.when((r < G - 1) if way == 0 else (r > 0))
            def _():
                for j in range(2):
                    zcopy(way, 0, j, i).start()

    def arrive(dist, i):
        for way in range(2):

            @pl.when((r >= dist) if way == 0 else (r <= G - 1 - dist))
            def _():
                q = r - dist if way == 0 else r + dist
                rows_q = at((G - 1 - q) * part + i * piece, piece, piece)
                ref = xt.at[:, rows_q, :]
                remote(ref, ref, z_s.at[way, dist - 1], z_r.at[way, dist - 1, i], to_x).wait_recv()

            if dist < G - 1:

                @pl.when(
                    jnp.logical_and(r >= dist, r < G - 1)
                    if way == 0
                    else jnp.logical_and(r <= G - 1 - dist, r > 0)
                )
                def _():
                    for j in range(2):
                        zcopy(way, dist, j, i).start()

    for t in range(nt):
        send_weights(t)
    for kind in range(4):
        load_own(kind, 0).start()

    spread_own(0)
    spread_own(1)
    for t in range(nt):
        for kind in range(4):
            load_own(kind, t).wait()
            s, g = kind // 2, kind % 2
            off, w = tiles[t][s]
            (wa, wb)[s][g, 0:width, off : off + w] = stage[kind, :, 0:w].astype(BF16)
            if t + 1 < nt:
                load_own(kind, t + 1).start()
    spread_own(2)
    for copy in swap1:
        copy.wait_recv()
    for j in range(G):
        ms[pl.ds(j * part, part), :] = get_stats(st, j * part, part)
    spread_own(3)
    for copy in gains:
        copy.wait_recv()

    def cast_d(t, carry):
        slot = lax.rem(t, 2)
        load_d(t, slot).wait()
        wd[tile_rows(t), :] = stage_d[slot].astype(BF16)

        @pl.when(t + 2 < ff // TILE)
        def _():
            load_d(t + 2, slot).start()

        return carry

    lax.fori_loop(0, ff // TILE, cast_d, 0)

    def normalize(k):
        slot = k % 2
        for i in range(2):
            rows_i = at(sets[k] * part + i * half, half, half)
            both = ms[rows_i, :]
            mean, inv = both[:, 0:1], both[:, 1:2]

            def norm(v, gain, bias):
                return ((v.astype(F32) - mean) * inv * gain + bias).astype(BF16)

            for lhs, j, side in ((la, 0, y), (lb, 1, x)):
                spot = at((i + side - 2 * i * side) * half, half, half)
                lhs[slot, spot, 0:width] = norm(tok[rows_i, :], ng[...], nb[...])
                lhs[slot, spot, width : 2 * width] = norm(xt[j, rows_i, :], gb[j, 0], gb[j, 1])

    ccopy = {}
    hcopy = {}
    for k in range(G):
        for t in range(nt):
            m = k * nt + t
            spot = pl.ds(k * half, half)
            for s in range(2):
                off, w = tiles[t][s]
                region = (ca, cb)[s].at[:, spot, pl.ds(off, w)]
                land = (ra, rb)[s].at[:, spot, pl.ds(off, w)]
                ccopy[m, s] = remote(region, land, c_s.at[s], c_r.at[s, m], (to_y, to_x)[s])
                side, who = ((y, x), (x, y))[s]
                cols = (a_cols, b_cols)[s]

                def block(side_, who_, lo, n):
                    return hid.at[at(sets[k] * part + side_ * half + lo, n, n), cols(t, who_)]

                own = block(side, who, 0, half)
                of_x = block(side, 1 - who, 0, half // 2) if s == 0 else block(1 - side, who, 0, half // 2)
                of_y = (
                    block(1 - side, who, half // 2, half // 2)
                    if s == 0
                    else block(side, 1 - who, half // 2, half // 2)
                )
                hcopy[m, s] = [
                    remote(own, own, h_s.at[s, 0], h_r.at[2 * s, m], to_x),
                    remote(own, own, h_s.at[s, 1], h_r.at[2 * s + 1, m], to_y),
                    remote(of_x, of_x, h_s.at[s, 2], h_r.at[4, m], to_y),
                    remote(of_y, of_y, h_s.at[s, 3], h_r.at[4, m], to_x),
                ]

    def scale_row(ref, s, t, who):
        off, w = tiles[t][s]
        first = (s * base_b + who * (na, nbw)[s] + off) // LANE
        return jnp.concatenate([ref[pl.ds(first + i, 1), :] for i in range(w // LANE)], axis=1)

    def s1(m):
        k, t = m // nt, m % nt
        for s in range(2):
            off, w = tiles[t][s]
            lhs, wgt, keep, away = ((la, wa, pa, ca), (lb, wb, pb, cb))[s]

            def one(g, carry):
                acc = jnp.dot(lhs[k % 2], wgt[g, :, off : off + w], preferred_element_type=F32)
                keep[g, k * half : (k + 1) * half, off : off + w] = acc[:half]
                away[g, k * half : (k + 1) * half, off : off + w] = acc[half:].astype(BF16)
                return carry

            lax.fori_loop(0, 2, one, 0)
            ccopy[m, s].start()

    def s2(m, sides=(0, 1)):
        k, t = m // nt, m % nt
        for s in sides:
            ccopy[m, s].wait_recv()
            off, w = tiles[t][s]
            keep, got = ((pa, ra), (pb, rb))[s]
            side, who = ((y, x), (x, y))[s]
            cols = (a_cols, b_cols)[s](t, who)
            spot = pl.ds(k * half, half)
            g = keep[0, spot, off : off + w] + got[0, spot, off : off + w].astype(F32)
            u = keep[1, spot, off : off + w] + got[1, spot, off : off + w].astype(F32)
            g = g * scale_row(gs, s, t, who)
            u = u * scale_row(us, s, t, who)
            h = (g / (1.0 + jnp.exp(-g)) * u).astype(BF16)
            hid[at(sets[k] * part + side * half, half, half), cols] = h
            hcopy[m, s][0].start()
            hcopy[m, s][1].start()

    def s3(m):
        for s in range(2):
            hcopy[m, s][0].wait_recv()
            hcopy[m, s][2].start()
            hcopy[m, s][1].wait_recv()
            hcopy[m, s][3].start()

    def out_cols(n):
        return pl.ds(pl.multiple_of(n * TILE, TILE), TILE)

    def to_inner(k, n):
        cols = out_cols(n)
        return remote(bp.at[k, :, cols], zs.at[k, :, cols], bp_s.at[k], zs_r.at[k, n], to_z[2])

    def to_owner(k, n):
        cols = out_cols(n)
        slot = k // 2
        return remote(bp.at[k, :, cols], zr.at[slot, :, cols], bp_s.at[k], bp_r.at[slot, n], to_z[k])

    def segments(t):
        (off_a, wid_a), (off_b, wid_b) = tiles[t]
        for who in range(2):
            yield who * na + off_a, wid_a
            yield base_b + who * nbw + off_b, wid_b

    def relays_in(m):
        (_, wid_a), (_, wid_b) = tiles[m % nt]
        ref = hid.at[pl.ds(0, half), pl.ds(0, wid_a + wid_b)]
        remote(ref, ref, h_s.at[0, 2], h_r.at[4, m], to_x).wait_recv()

    nn = width // TILE

    def s4(k, first, last):
        if first == 0:
            for t in range(nt):
                relays_in(k * nt + t)
        lhs = at(sets[k] * part, part, part)

        def body(n, carry):
            cols = out_cols(n)
            bp[k, :, cols] = jnp.dot(hid[lhs, :], wd[:, cols], preferred_element_type=F32).astype(BF16)
            if k == G - 2:
                to_owner(k, n).start()
            else:

                @pl.when(jnp.logical_not(inner))
                def _():
                    to_inner(k, n).start()

            return carry

        lax.fori_loop(first, last, body, 0)

    def partial(lhs, cols, steps_in):
        return sum(
            jnp.dot(hid[lhs, lo : lo + w], wd[lo : lo + w, cols], preferred_element_type=F32)
            for t in steps_in
            for lo, w in segments(t)
        )

    def s4_head(k):
        for t in range(nt - 1):
            relays_in(k * nt + t)
        lhs = at(sets[k] * part, part, part)

        def body(n, carry):
            cols = out_cols(n)
            mix[:, cols] = partial(lhs, cols, range(nt - 1))
            return carry

        lax.fori_loop(0, nn, body, 0)

    def s4_tail(k):
        relays_in(k * nt + nt - 1)
        lhs = at(sets[k] * part, part, part)
        for n in range(nn):
            cols = out_cols(n)
            acc = mix[:, cols] + partial(lhs, cols, (nt - 1,))
            bp[k, :, cols] = acc.astype(BF16)
            to_owner(k, n).start()

    def join(k):
        @pl.when(inner)
        def _():
            def body(n, carry):
                cols = out_cols(n)
                to_inner(k, n).wait_recv()
                bp[k, :, cols] = (bp[k, :, cols].astype(F32) + zs[k, :, cols].astype(F32)).astype(BF16)
                to_owner(k, n).start()
                return carry

            lax.fori_loop(0, nn, body, 0)

    def s5(t):
        relays_in((G - 1) * nt + t)
        lhs = at(sets[G - 1] * part, part, part)
        late = t == nt - 1
        for n in range(nn):
            cols = pl.ds(n * TILE, TILE)
            acc = partial(lhs, cols, (t,))
            if t > 0:
                acc = acc + mix[:, cols]
            if late:
                for slot, k in ((0, 0), (1, 2)):
                    to_owner(k, n).wait_recv()
                    acc = acc + zr[slot, :, cols].astype(F32)
            if late:
                acc = acc * down_scale[:, cols]
                for i in range(2):
                    spot = at((i + y - 2 * i * y) * half, half, half)
                    mix[i * half : (i + 1) * half, cols] = (
                        0.5 * la[(G - 1) % 2, spot, cols].astype(F32) + acc[i * half : (i + 1) * half]
                    )
            else:
                mix[:, cols] = acc

    def weights_in(t):
        for s in range(2):
            wcopy[t, s].wait_recv()
            fcopy[t, s].start()

    def weights_ready(t):
        for s in range(2):
            fcopy[t, s].wait_recv()

    steps = G * nt
    first = 2 * nt

    for i in range(PIECES - 1):
        arrive(1, i)
    weights_in(0)
    arrive(1, PIECES - 1)
    normalize(0)
    normalize(1)
    weights_ready(0)
    s1(0)
    s1(nt)
    for t in range(1, nt):
        if t == nt - 1:
            s2(0, (0,))
        weights_in(t)
        weights_ready(t)
        s1(t)
        if t == nt - 1:
            s2(0, (1,))
        s1(nt + t)
        for j in range(PIECES):
            if 1 + j * (nt - 1) // PIECES == t:
                arrive(2, j)
    for i in range(2, first):
        if i == first - 1:
            normalize(2)
            s1(first)
        s2(i - 1)
        s3(i - 2)
    s4(0, 0, nn)

    for i in range(first, steps + 3):
        border = i == steps - nt
        if border:
            s2(i - 1)
        if i < steps and i > first:
            if border:
                for j in range(PIECES):
                    arrive(G - 1, j)
                normalize(G - 1)
            s1(i)
        k = i // nt - 1
        edge = i % nt == nt - 1 and k < G - 1
        early = i == steps - nt + 1
        if early:
            s3(i - 2)
        if edge and k == 2:
            s4_head(2)
        if not border and i - 1 < steps:
            s2(i - 1)
        if edge and k == 2:
            join(1)
            s4_tail(2)
        if not early and i - 2 < steps:
            s3(i - 2)
        if edge:
            if k < 2:
                s4(k, 0, nn)
            if k == 1:
                join(0)
        if i >= steps and i - steps < nt:
            s5(i - steps)

    put_stats(mix[...], st2, 0)
    swap2 = swap_stats(st2, 1)
    for copy in swap2:
        copy.start()
    for copy in swap1 + gains:
        copy.wait_send()
    for k in range(G - 1):
        remote(bp.at[k], bp.at[k], bp_s.at[k], bp_r.at[0, 0], to_x).wait_send()
    for j in range(2):
        ref = tok.at[pl.ds(0, part), :]
        remote(ref, ref, tok_s.at[j], tok_r.at[j, 0], to_x).wait_send()
    for s in range(2):
        mine, away = ((sa, ca), (sb, cb))[s]
        remote(mine, mine, w_s.at[s], w_r.at[0, s], to_x).wait_send()
        remote(mine, mine, f_s.at[s], f_r.at[0, s], to_x).wait_send()
        remote(away, away, c_s.at[s], c_r.at[s, 0], to_x).wait_send()
        for i in range(4):
            ref = away.at[0] if i < 2 else away.at[0, pl.ds(0, rows // 4)]
            remote(ref, ref, h_s.at[s, i], h_r.at[4, 0], to_x).wait_send()
    for way in range(2):
        for dist in range(G - 1):

            @pl.when(
                jnp.logical_and(r >= dist, r < G - 1)
                if way == 0
                else jnp.logical_and(r <= G - 1 - dist, r > 0)
            )
            def _():
                ref = xt.at[:, pl.ds(0, part), :]
                remote(ref, ref, z_s.at[way, dist], z_r.at[way, dist, 0], to_x).wait_send()
    for copy in swap2:
        copy.wait_recv()
    both = get_stats(st2, 0, part)
    for i in range(2):
        spot = pl.ds(i * half, half)
        mean, inv = both[i * half : (i + 1) * half, 0:1], both[i * half : (i + 1) * half, 1:2]
        out[spot, :] = ((mix[spot, :] - mean) * inv * og[...] + ob[...]).astype(BF16)

    for copy in swap2:
        copy.wait_send()


def fused(
    tokens,
    norm_gain,
    norm_bias,
    gate_weight,
    up_weight,
    gate_scale,
    up_scale,
    down_weight,
    down_scale,
    out_gain,
    out_bias,
):
    rows, width = tokens.shape
    ff = gate_weight.shape[1]
    na, nbw, tiles = tiles_of(ff)
    nt = len(tiles)
    part = rows // G
    half = part // 2
    kh = width // 2
    steps = G * nt
    hbm = pl.BlockSpec(memory_space=pl.ANY)
    row = lambda v: v.reshape(1, -1)
    dma = pltpu.SemaphoreType.DMA
    return pl.pallas_call(
        kernel,
        out_shape=pltpu.VMEM((part, width), BF16),
        in_specs=[hbm] * 11,
        out_specs=pl.BlockSpec(memory_space=pltpu.VMEM),
        scratch_shapes=[
            pltpu.VMEM((rows, width), BF16),
            pltpu.VMEM((1, width), F32),
            pltpu.VMEM((1, width), F32),
            pltpu.VMEM((ff // LANE, LANE), F32),
            pltpu.VMEM((ff // LANE, LANE), F32),
            pltpu.VMEM((1, width), F32),
            pltpu.VMEM((1, width), F32),
            pltpu.VMEM((1, width), F32),
            pltpu.VMEM((4, width, TILE), F32),
            pltpu.VMEM((2, TILE, width), F32),
            pltpu.VMEM((2, 2 * width, na), BF16),
            pltpu.VMEM((2, 2 * width, nbw), BF16),
            pltpu.VMEM((2, kh, na), BF16),
            pltpu.VMEM((2, kh, nbw), BF16),
            pltpu.VMEM((2, rows, width), BF16),
            pltpu.VMEM((2, 2, 1, width), F32),
            pltpu.VMEM((2, part, 2 * width), BF16),
            pltpu.VMEM((2, part, 2 * width), BF16),
            pltpu.VMEM((2, rows // 2, na), F32),
            pltpu.VMEM((2, rows // 2, nbw), F32),
            pltpu.VMEM((2, rows // 2, na), BF16),
            pltpu.VMEM((2, rows // 2, nbw), BF16),
            pltpu.VMEM((2, rows // 2, na), BF16),
            pltpu.VMEM((2, rows // 2, nbw), BF16),
            pltpu.VMEM((rows, ff), BF16),
            pltpu.VMEM((ff, width), BF16),
            pltpu.VMEM((G - 1, part, width), BF16),
            pltpu.VMEM((2, part, width), BF16),
            pltpu.VMEM((2, part, width), BF16),
            pltpu.VMEM((part, width), F32),
            pltpu.VMEM((rows, LANE), F32),
            pltpu.VMEM((G, 8, rows), F32),
            pltpu.VMEM((G, 8, part), F32),
            dma((G + 7,)),
            dma((4, 2)),
            dma((2,)),
            dma((2,)),
            dma((2, PIECES)),
            dma((2, G - 1)),
            dma((2, G - 1, PIECES)),
            dma((2, 2)),
            dma((2, 2)),
            dma((2,)),
            dma((nt, 2)),
            dma((2,)),
            dma((nt, 2)),
            dma((2,)),
            dma((2, steps)),
            dma((2, 4)),
            dma((5, steps)),
            dma((G - 1,)),
            dma((2, width // TILE)),
            dma((2, width // TILE)),
            dma((2, G - 1)),
            dma((2, G - 1)),
        ],
        compiler_params=pltpu.CompilerParams(
            collective_id=0, has_side_effects=True, vmem_limit_bytes=63500000
        ),
    )(
        tokens,
        row(norm_gain),
        row(norm_bias),
        gate_weight,
        up_weight,
        gate_scale.reshape(-1, LANE),
        up_scale.reshape(-1, LANE),
        down_weight,
        row(down_scale),
        row(out_gain),
        row(out_bias),
    )


def local(*args):
    rows, width = args[0].shape
    ff = args[3].shape[1]
    fits = (
        lax.axis_size("cb") == G
        and lax.axis_size("ra") == G
        and lax.axis_size("dp") == 2
        and rows % (256 * G) == 0
        and width % TILE == 0
        and ff % TILE == 0
        and min(pair[1][1] for pair in tiles_of(ff)[2]) > 0
        and rows * width <= 1 << 20
        and ff * width <= 2816 * 1024
    )
    return (fused if fits else plain)(*args)


def solution(mesh):
    return jax.shard_map(
        local,
        mesh=mesh,
        in_specs=(
            P("dp", "cb"),
            P("cb"),
            P("cb"),
            P("cb", "ra"),
            P("cb", "ra"),
            P("ra"),
            P("ra"),
            P("ra", "cb"),
            P("cb"),
            P("cb"),
            P("cb"),
        ),
        out_specs=P(("dp", "ra"), "cb"),
        check_vma=False,
    )
```

```python
import jax
import jax.numpy as jnp
from jax import lax
from jax.experimental import pallas as pl
from jax.experimental.pallas import tpu as pltpu
from jax.sharding import PartitionSpec as P

MESH = pl.DeviceIdType.MESH
EPS = 1e-05
TILE = 256
LANE = 128
PIECES = 4
G = 4
F32 = jnp.float32
BF16 = jnp.bfloat16


def standardize(values):
    width = values.shape[1] * lax.axis_size("cb")
    total = lax.psum(jnp.sum(values, axis=1), "cb")
    mean = total / width
    centred = values - mean[:, None]
    spread = lax.psum(jnp.sum(centred * centred, axis=1), "cb") / width
    return centred * lax.rsqrt(spread + EPS)[:, None]


def plain(
    tokens,
    norm_gain,
    norm_bias,
    gate_weight,
    up_weight,
    gate_scale,
    up_scale,
    down_weight,
    down_scale,
    out_gain,
    out_bias,
):
    normed = (standardize(tokens.astype(F32)) * norm_gain + norm_bias).astype(BF16)
    gate_part = jnp.dot(normed, gate_weight.astype(BF16), preferred_element_type=F32)
    up_part = jnp.dot(normed, up_weight.astype(BF16), preferred_element_type=F32)
    gate_share, up_share = (
        lax.psum_scatter(part.astype(BF16), "cb", scatter_dimension=1, tiled=True).astype(F32)
        for part in (gate_part, up_part)
    )
    share = gate_share.shape[1]
    offset = lax.axis_index("cb") * share
    gate_cols = lax.dynamic_slice_in_dim(gate_scale, offset, share, 0)
    up_cols = lax.dynamic_slice_in_dim(up_scale, offset, share, 0)
    hidden_share = (jax.nn.silu(gate_share * gate_cols) * (up_share * up_cols)).astype(BF16)
    hidden = lax.all_gather(hidden_share, "cb", axis=1, tiled=True)
    own_rows = hidden.shape[0] // lax.axis_size("ra")
    part = jnp.dot(hidden, down_weight.astype(BF16), preferred_element_type=F32)
    branch = lax.psum_scatter(part, "ra", scatter_dimension=0, tiled=True) * down_scale
    own_normed = lax.dynamic_slice_in_dim(normed, lax.axis_index("ra") * own_rows, own_rows, 0)
    mixed = 0.5 * own_normed.astype(F32) + branch
    return (standardize(mixed) * out_gain + out_bias).astype(BF16)


def tiles_of(ff):
    wide = (ff // LANE + 3) // 4 * LANE
    narrow = ff // 2 - wide
    count = (wide + TILE - 1) // TILE
    both = []
    for t in range(count):
        off = t * TILE
        both.append(((off, min(TILE, wide - off)), (off, min(TILE, narrow - off))))
    return wide, narrow, both


def kernel(
    tok_hbm,
    ng_hbm,
    nb_hbm,
    gw,
    uw,
    gs_hbm,
    us_hbm,
    dw,
    ds_hbm,
    og_hbm,
    ob_hbm,
    out,
    tok,
    ng,
    nb,
    gs,
    us,
    down_scale,
    og,
    ob,
    stage,
    stage_d,
    wa,
    wb,
    sa,
    sb,
    xt,
    gb,
    la,
    lb,
    pa,
    pb,
    ca,
    cb,
    ra,
    rb,
    hid,
    wd,
    bp,
    zr,
    zs,
    mix,
    ms,
    st,
    st2,
    in_sem,
    stage_sem,
    stage_d_sem,
    tok_s,
    tok_r,
    z_s,
    z_r,
    gb_s,
    gb_r,
    w_s,
    w_r,
    f_s,
    f_r,
    c_s,
    c_r,
    h_s,
    h_r,
    bp_s,
    bp_r,
    zs_r,
    st_s,
    st_r,
):
    rows, width = tok.shape
    ff = gw.shape[1]
    na, nbw, tiles = tiles_of(ff)
    nt = len(tiles)
    base_b = 2 * na
    part = rows // G
    half = part // 2
    piece = part // PIECES
    kh = width // 2
    full = float(width * G)

    b = lax.axis_index("cb")
    r = lax.axis_index("ra")
    p = lax.axis_index("dp")
    x = lax.rem(b, 2)
    y = b // 2
    to_x = {"cb": b + 1 - 2 * x}
    to_y = {"cb": b + 2 - 4 * y}
    to_d = {"cb": (G - 1) - b}
    twin = {"dp": 1 - p}
    hi = r // 2
    sets = [3 - 3 * hi, 2 - hi, r + 1 - 2 * lax.rem(r, 2), r]
    inner = lax.rem(r, 2) + hi == 1
    to_z = [{"ra": s} for s in sets[:3]]
    ring = [{"ra": lax.rem(r + o, G)} for o in range(1, G)]

    barrier = pltpu.get_barrier_semaphore()
    greet = [to_x, to_y, to_d, twin] + ring
    for peer in greet:
        pl.semaphore_signal(barrier, inc=1, device_id=peer, device_id_type=MESH)

    small = [
        pltpu.make_async_copy(src, dst, in_sem.at[G + i])
        for i, (src, dst) in enumerate(
            (
                (ng_hbm, ng),
                (nb_hbm, nb),
                (gs_hbm, gs),
                (us_hbm, us),
                (ds_hbm, down_scale),
                (og_hbm, og),
                (ob_hbm, ob),
            )
        )
    ]
    tok_in = [
        pltpu.make_async_copy(
            tok_hbm.at[pl.ds(pl.multiple_of(q * part, part), part), :],
            tok.at[pl.ds(pl.multiple_of(q * part, part), part), :],
            in_sem.at[j],
        )
        for j, q in enumerate(lax.rem(G - 1 - r + j, G) for j in range(G))
    ]
    for copy in tok_in + small:
        copy.start()

    def at(start, size, align):
        return pl.ds(pl.multiple_of(start, align), size)

    def remote(src, dst, send, recv, peer):
        return pltpu.make_async_remote_copy(
            src_ref=src,
            dst_ref=dst,
            send_sem=send,
            recv_sem=recv,
            device_id=peer,
            device_id_type=MESH,
        )

    def a_cols(t, who):
        off, w = tiles[t][0]
        return at(who * na + off, w, LANE)

    def b_cols(t, who):
        off, w = tiles[t][1]
        return at(base_b + who * nbw + off, w, LANE)

    def load_send(kind, t):
        slot = t % 2
        src = (gw, uw)[kind % 2]
        cols = a_cols(t, 1 - x) if kind < 2 else b_cols(t, 1 - y)
        w = tiles[t][kind // 2][1]
        return pltpu.make_async_copy(
            src.at[at(p * kh, kh, kh), cols],
            stage.at[kind, pl.ds(slot * kh, kh), pl.ds(0, w)],
            stage_sem.at[kind, slot],
        )

    def load_own(kind, t):
        src = (gw, uw)[kind % 2]
        cols = a_cols(t, x) if kind < 2 else b_cols(t, y)
        w = tiles[t][kind // 2][1]
        return pltpu.make_async_copy(
            src.at[:, cols], stage.at[kind, :, pl.ds(0, w)], stage_sem.at[kind, 0]
        )

    def tile_rows(t):
        return pl.ds(pl.multiple_of(t * TILE, TILE), TILE)

    def load_d(t, slot):
        return pltpu.make_async_copy(dw.at[tile_rows(t), :], stage_d.at[slot], stage_d_sem.at[slot])

    for t in range(min(2, nt)):
        for kind in range(4):
            load_send(kind, t).start()
    for t in range(2):
        load_d(t, t).start()

    tok_in[0].wait()
    pl.semaphore_wait(barrier, len(greet))

    own_tok = []
    for i in range(PIECES):
        rows_i = at((G - 1 - r) * part + i * piece, piece, piece)
        for j, peer in enumerate((to_x, to_y)):
            own_tok.append(
                remote(tok.at[rows_i, :], xt.at[j, rows_i, :], tok_s.at[j], tok_r.at[j, i], peer)
            )
    for copy in own_tok:
        copy.start()
    for copy in tok_in[1:] + small:
        copy.wait()

    def put_stats(v, dst, col):
        total = jnp.sum(v, axis=1, keepdims=True)
        off = v - total * (1.0 / width)
        spread = jnp.sum(off * off, axis=1, keepdims=True)
        lane = lax.broadcasted_iota(jnp.int32, (v.shape[0], LANE), 1)
        both = jnp.where(lane == 0, total, spread)
        dst[0, :, pl.ds(col, v.shape[0])] = both.T[:8, :]

    def get_stats(src, col, n):
        parts = [src[i, 0:2, pl.ds(col, n)] for i in range(G)]
        mean = (parts[0][0:1] + parts[1][0:1] + parts[2][0:1] + parts[3][0:1]) / full
        spread = jnp.zeros_like(mean)
        for q in parts:
            d = q[0:1] * (1.0 / width) - mean
            spread = spread + q[1:2] + width * (d * d)
        inv = lax.rsqrt(spread / full + EPS)
        sub = lax.broadcasted_iota(jnp.int32, (LANE, n), 0)
        return jnp.where(sub == 0, mean, inv).T

    def swap_stats(buf, which):
        return [
            remote(buf.at[0, pl.ds(0, 2)], buf.at[1 + i, pl.ds(0, 2)], st_s.at[which, i], st_r.at[which, i], peer)
            for i, peer in enumerate((to_x, to_y, to_d))
        ]

    for j in range(G):
        put_stats(tok[pl.ds(j * part, part), :].astype(F32), st, j * part)
    swap1 = swap_stats(st, 0)
    for copy in swap1:
        copy.start()
    gains = []
    for j, peer in enumerate((to_x, to_y)):
        for i, ref in enumerate((ng, nb)):
            gains.append(remote(ref, gb.at[j, i], gb_s.at[0], gb_r.at[0], peer))
    for copy in gains:
        copy.start()

    wcopy = {}
    fcopy = {}
    for t in range(nt):
        for s in range(2):
            off, w = tiles[t][s]
            mine = (sa, sb)[s].at[:, :, pl.ds(off, w)]
            there = (wa, wb)[s].at[:, at(width + p * kh, kh, kh), pl.ds(off, w)]
            wcopy[t, s] = remote(mine, there, w_s.at[s], w_r.at[t, s], (to_x, to_y)[s])
            fcopy[t, s] = remote(there, there, f_s.at[s], f_r.at[t, s], twin)

    def send_weights(t):
        for kind in range(4):
            load_send(kind, t).wait()
            s, g = kind // 2, kind % 2
            off, w = tiles[t][s]
            (sa, sb)[s][g, :, off : off + w] = stage[kind, (t % 2) * kh : (t % 2 + 1) * kh, 0:w].astype(BF16)
            if t + 2 < nt:
                load_send(kind, t + 2).start()
        for s in range(2):
            wcopy[t, s].start()

    def zcopy(way, dist, j, i):
        q = r - dist if way == 0 else r + dist
        rows_q = at((G - 1 - q) * part + i * piece, piece, piece)
        ref = xt.at[j, rows_q, :]
        peer = {"ra": r + 1 if way == 0 else r - 1}
        return remote(ref, ref, z_s.at[way, dist], z_r.at[way, dist, i], peer)

    def spread_own(i):
        for j in range(2):
            own_tok[2 * i + j].wait_recv()
        for way in range(2):

            @pl.when((r < G - 1) if way == 0 else (r > 0))
            def _():
                for j in range(2):
                    zcopy(way, 0, j, i).start()

    def arrive(dist, i):
        for way in range(2):

            @pl.when((r >= dist) if way == 0 else (r <= G - 1 - dist))
            def _():
                q = r - dist if way == 0 else r + dist
                rows_q = at((G - 1 - q) * part + i * piece, piece, piece)
                ref = xt.at[:, rows_q, :]
                remote(ref, ref, z_s.at[way, dist - 1], z_r.at[way, dist - 1, i], to_x).wait_recv()

            if dist < G - 1:

                @pl.when(
                    jnp.logical_and(r >= dist, r < G - 1)
                    if way == 0
                    else jnp.logical_and(r <= G - 1 - dist, r > 0)
                )
                def _():
                    for j in range(2):
                        zcopy(way, dist, j, i).start()

    for t in range(nt):
        send_weights(t)
    for kind in range(4):
        load_own(kind, 0).start()

    spread_own(0)
    spread_own(1)
    for t in range(nt):
        for kind in range(4):
            load_own(kind, t).wait()
            s, g = kind // 2, kind % 2
            off, w = tiles[t][s]
            (wa, wb)[s][g, 0:width, off : off + w] = stage[kind, :, 0:w].astype(BF16)
            if t + 1 < nt:
                load_own(kind, t + 1).start()
    spread_own(2)
    for copy in swap1:
        copy.wait_recv()
    for j in range(G):
        ms[pl.ds(j * part, part), :] = get_stats(st, j * part, part)
    spread_own(3)
    remote(gb, gb, gb_s.at[0], gb_r.at[0], to_x).wait_recv()

    def cast_d(t, carry):
        slot = lax.rem(t, 2)
        load_d(t, slot).wait()
        wd[tile_rows(t), :] = stage_d[slot].astype(BF16)

        @pl.when(t + 2 < ff // TILE)
        def _():
            load_d(t + 2, slot).start()

        return carry

    lax.fori_loop(0, ff // TILE, cast_d, 0)

    def normalize(k):
        slot = k % 2
        for i in range(2):
            rows_i = at(sets[k] * part + i * half, half, half)
            both = ms[rows_i, :]
            mean, inv = both[:, 0:1], both[:, 1:2]

            def norm(v, gain, bias):
                return ((v.astype(F32) - mean) * inv * gain + bias).astype(BF16)

            for lhs, j, side in ((la, 0, y), (lb, 1, x)):
                spot = at((i + side - 2 * i * side) * half, half, half)
                lhs[slot, spot, 0:width] = norm(tok[rows_i, :], ng[...], nb[...])
                lhs[slot, spot, width : 2 * width] = norm(xt[j, rows_i, :], gb[j, 0], gb[j, 1])

    ccopy = {}
    hcopy = {}
    for k in range(G):
        for t in range(nt):
            m = k * nt + t
            spot = pl.ds(k * half, half)
            for s in range(2):
                off, w = tiles[t][s]
                region = (ca, cb)[s].at[:, spot, pl.ds(off, w)]
                land = (ra, rb)[s].at[:, spot, pl.ds(off, w)]
                ccopy[m, s] = remote(region, land, c_s.at[s], c_r.at[s, m], (to_y, to_x)[s])
                side, who = ((y, x), (x, y))[s]
                cols = (a_cols, b_cols)[s]

                def block(side_, who_, lo, n):
                    return hid.at[at(sets[k] * part + side_ * half + lo, n, n), cols(t, who_)]

                own = block(side, who, 0, half)
                of_x = block(side, 1 - who, 0, half // 2) if s == 0 else block(1 - side, who, 0, half // 2)
                of_y = (
                    block(1 - side, who, half // 2, half // 2)
                    if s == 0
                    else block(side, 1 - who, half // 2, half // 2)
                )
                hcopy[m, s] = [
                    remote(own, own, h_s.at[s, 0], h_r.at[0, m], to_x),
                    remote(own, own, h_s.at[s, 1], h_r.at[1, m], to_y),
                    remote(of_x, of_x, h_s.at[s, 2], h_r.at[2, m], to_y),
                    remote(of_y, of_y, h_s.at[s, 3], h_r.at[2, m], to_x),
                ]

    def scale_row(ref, s, t, who):
        off, w = tiles[t][s]
        first = (s * base_b + who * (na, nbw)[s] + off) // LANE
        return jnp.concatenate([ref[pl.ds(first + i, 1), :] for i in range(w // LANE)], axis=1)

    def s1(m):
        k, t = m // nt, m % nt
        for s in range(2):
            off, w = tiles[t][s]
            lhs, wgt, keep, away = ((la, wa, pa, ca), (lb, wb, pb, cb))[s]

            def one(g, carry):
                acc = jnp.dot(lhs[k % 2], wgt[g, :, off : off + w], preferred_element_type=F32)
                keep[g, k * half : (k + 1) * half, off : off + w] = acc[:half]
                away[g, k * half : (k + 1) * half, off : off + w] = acc[half:].astype(BF16)
                return carry

            lax.fori_loop(0, 2, one, 0)
            ccopy[m, s].start()

    def s2(m, sides=(0, 1)):
        k, t = m // nt, m % nt
        for s in sides:
            ccopy[m, s].wait_recv()
            off, w = tiles[t][s]
            keep, got = ((pa, ra), (pb, rb))[s]
            side, who = ((y, x), (x, y))[s]
            cols = (a_cols, b_cols)[s](t, who)
            spot = pl.ds(k * half, half)
            g = keep[0, spot, off : off + w] + got[0, spot, off : off + w].astype(F32)
            u = keep[1, spot, off : off + w] + got[1, spot, off : off + w].astype(F32)
            g = g * scale_row(gs, s, t, who)
            u = u * scale_row(us, s, t, who)
            h = (g / (1.0 + jnp.exp(-g)) * u).astype(BF16)
            hid[at(sets[k] * part + side * half, half, half), cols] = h
            hcopy[m, s][0].start()
            hcopy[m, s][1].start()

    def s3(m):
        (_, wid_a), (_, wid_b) = tiles[m % nt]
        ref = hid.at[pl.ds(0, half), pl.ds(0, wid_a + wid_b)]
        for i in range(2):
            remote(ref, ref, h_s.at[0, i], h_r.at[i, m], to_x).wait_recv()
            for s in range(2):
                hcopy[m, s][2 + i].start()

    def out_cols(n):
        return pl.ds(pl.multiple_of(n * TILE, TILE), TILE)

    def to_inner(k, n):
        cols = out_cols(n)
        return remote(bp.at[k, :, cols], zs.at[k, :, cols], bp_s.at[k], zs_r.at[k, n], to_z[2])

    def to_owner(k, n):
        cols = out_cols(n)
        slot = k // 2
        return remote(bp.at[k, :, cols], zr.at[slot, :, cols], bp_s.at[k], bp_r.at[slot, n], to_z[k])

    def segments(t):
        (off_a, wid_a), (off_b, wid_b) = tiles[t]
        for who in range(2):
            yield who * na + off_a, wid_a
            yield base_b + who * nbw + off_b, wid_b

    def relays_in(m):
        (_, wid_a), (_, wid_b) = tiles[m % nt]
        ref = hid.at[pl.ds(0, half), pl.ds(0, wid_a + wid_b)]
        remote(ref, ref, h_s.at[0, 2], h_r.at[2, m], to_x).wait_recv()

    nn = width // TILE

    def s4(k, first, last):
        if first == 0:
            for t in range(nt):
                relays_in(k * nt + t)
        lhs = at(sets[k] * part, part, part)

        def body(n, carry):
            cols = out_cols(n)
            bp[k, :, cols] = jnp.dot(hid[lhs, :], wd[:, cols], preferred_element_type=F32).astype(BF16)
            if k == G - 2:
                to_owner(k, n).start()
            else:

                @pl.when(jnp.logical_not(inner))
                def _():
                    to_inner(k, n).start()

            return carry

        lax.fori_loop(first, last, body, 0)

    def partial(lhs, cols, steps_in):
        return sum(
            jnp.dot(hid[lhs, lo : lo + w], wd[lo : lo + w, cols], preferred_element_type=F32)
            for t in steps_in
            for lo, w in segments(t)
        )

    def s4_head(k):
        for t in range(nt - 1):
            relays_in(k * nt + t)
        lhs = at(sets[k] * part, part, part)

        def body(n, carry):
            cols = out_cols(n)
            mix[:, cols] = partial(lhs, cols, range(nt - 1))
            return carry

        lax.fori_loop(0, nn, body, 0)

    def s4_tail(k):
        relays_in(k * nt + nt - 1)
        lhs = at(sets[k] * part, part, part)
        for n in range(nn):
            cols = out_cols(n)
            acc = mix[:, cols] + partial(lhs, cols, (nt - 1,))
            bp[k, :, cols] = acc.astype(BF16)
            to_owner(k, n).start()

    def join(k):
        @pl.when(inner)
        def _():
            def body(n, carry):
                cols = out_cols(n)
                to_inner(k, n).wait_recv()
                bp[k, :, cols] = (bp[k, :, cols].astype(F32) + zs[k, :, cols].astype(F32)).astype(BF16)
                to_owner(k, n).start()
                return carry

            lax.fori_loop(0, nn, body, 0)

    def s5(t):
        relays_in((G - 1) * nt + t)
        lhs = at(sets[G - 1] * part, part, part)
        late = t == nt - 1
        for n in range(nn):
            cols = pl.ds(n * TILE, TILE)
            acc = partial(lhs, cols, (t,))
            if t > 0:
                acc = acc + mix[:, cols]
            if late:
                for slot, k in ((0, 0), (1, 2)):
                    to_owner(k, n).wait_recv()
                    acc = acc + zr[slot, :, cols].astype(F32)
            if late:
                acc = acc * down_scale[:, cols]
                for i in range(2):
                    spot = at((i + y - 2 * i * y) * half, half, half)
                    mix[i * half : (i + 1) * half, cols] = (
                        0.5 * la[(G - 1) % 2, spot, cols].astype(F32) + acc[i * half : (i + 1) * half]
                    )
            else:
                mix[:, cols] = acc

    def weights_in(t):
        for s in range(2):
            wcopy[t, s].wait_recv()
            fcopy[t, s].start()

    def weights_ready(t):
        for s in range(2):
            fcopy[t, s].wait_recv()

    steps = G * nt
    first = 2 * nt

    for i in range(PIECES - 1):
        arrive(1, i)
    weights_in(0)
    arrive(1, PIECES - 1)
    normalize(0)
    normalize(1)
    weights_ready(0)
    s1(0)
    s1(nt)
    for t in range(1, nt):
        if t == nt - 1:
            s2(0, (0,))
        weights_in(t)
        weights_ready(t)
        s1(t)
        if t == nt - 1:
            s2(0, (1,))
        s1(nt + t)
        for j in range(PIECES):
            if 1 + j * (nt - 1) // PIECES == t:
                arrive(2, j)
    for i in range(2, first):
        if i == first - 1:
            normalize(2)
            s1(first)
        s2(i - 1)
        s3(i - 2)
    s4(0, 0, nn)

    for i in range(first, steps + 3):
        border = i == steps - nt
        if border:
            s2(i - 1)
        if i < steps and i > first:
            if border:
                for j in range(PIECES):
                    arrive(G - 1, j)
                normalize(G - 1)
            s1(i)
        k = i // nt - 1
        edge = i % nt == nt - 1 and k < G - 1
        early = i == steps - nt + 1
        if early:
            s3(i - 2)
        if edge and k == 2:
            s4_head(2)
        if not border and i - 1 < steps:
            s2(i - 1)
        if edge and k == 2:
            join(1)
            s4_tail(2)
        if not early and i - 2 < steps:
            s3(i - 2)
        if edge:
            if k < 2:
                s4(k, 0, nn)
            if k == 1:
                join(0)
        if i >= steps and i - steps < nt:
            s5(i - steps)

    put_stats(mix[...], st2, 0)
    swap2 = swap_stats(st2, 1)
    for copy in swap2:
        copy.start()
    for copy in swap1:
        copy.wait_send()
    remote(gb, gb, gb_s.at[0], gb_r.at[0], to_x).wait_send()
    for k in range(G - 1):
        remote(bp.at[k], bp.at[k], bp_s.at[k], bp_r.at[0, 0], to_x).wait_send()
    for j in range(2):
        ref = tok.at[pl.ds(0, part), :]
        remote(ref, ref, tok_s.at[j], tok_r.at[j, 0], to_x).wait_send()
    for s in range(2):
        mine, away = ((sa, ca), (sb, cb))[s]
        remote(mine, mine, w_s.at[s], w_r.at[0, s], to_x).wait_send()
        remote(mine, mine, f_s.at[s], f_r.at[0, s], to_x).wait_send()
        remote(away, away, c_s.at[s], c_r.at[s, 0], to_x).wait_send()
        for i in range(4):
            ref = away.at[0] if i < 2 else away.at[0, pl.ds(0, rows // 4)]
            remote(ref, ref, h_s.at[s, i], h_r.at[2, 0], to_x).wait_send()
    for way in range(2):
        for dist in range(G - 1):

            @pl.when(
                jnp.logical_and(r >= dist, r < G - 1)
                if way == 0
                else jnp.logical_and(r <= G - 1 - dist, r > 0)
            )
            def _():
                ref = xt.at[:, pl.ds(0, part), :]
                remote(ref, ref, z_s.at[way, dist], z_r.at[way, dist, 0], to_x).wait_send()
    for copy in swap2:
        copy.wait_recv()
    both = get_stats(st2, 0, part)
    for i in range(2):
        spot = pl.ds(i * half, half)
        mean, inv = both[i * half : (i + 1) * half, 0:1], both[i * half : (i + 1) * half, 1:2]
        out[spot, :] = ((mix[spot, :] - mean) * inv * og[...] + ob[...]).astype(BF16)

    for copy in swap2:
        copy.wait_send()


def fused(
    tokens,
    norm_gain,
    norm_bias,
    gate_weight,
    up_weight,
    gate_scale,
    up_scale,
    down_weight,
    down_scale,
    out_gain,
    out_bias,
):
    rows, width = tokens.shape
    ff = gate_weight.shape[1]
    na, nbw, tiles = tiles_of(ff)
    nt = len(tiles)
    part = rows // G
    half = part // 2
    kh = width // 2
    steps = G * nt
    hbm = pl.BlockSpec(memory_space=pl.ANY)
    row = lambda v: v.reshape(1, -1)
    dma = pltpu.SemaphoreType.DMA
    return pl.pallas_call(
        kernel,
        out_shape=pltpu.VMEM((part, width), BF16),
        in_specs=[hbm] * 11,
        out_specs=pl.BlockSpec(memory_space=pltpu.VMEM),
        scratch_shapes=[
            pltpu.VMEM((rows, width), BF16),
            pltpu.VMEM((1, width), F32),
            pltpu.VMEM((1, width), F32),
            pltpu.VMEM((ff // LANE, LANE), F32),
            pltpu.VMEM((ff // LANE, LANE), F32),
            pltpu.VMEM((1, width), F32),
            pltpu.VMEM((1, width), F32),
            pltpu.VMEM((1, width), F32),
            pltpu.VMEM((4, width, TILE), F32),
            pltpu.VMEM((2, TILE, width), F32),
            pltpu.VMEM((2, 2 * width, na), BF16),
            pltpu.VMEM((2, 2 * width, nbw), BF16),
            pltpu.VMEM((2, kh, na), BF16),
            pltpu.VMEM((2, kh, nbw), BF16),
            pltpu.VMEM((2, rows, width), BF16),
            pltpu.VMEM((2, 2, 1, width), F32),
            pltpu.VMEM((2, part, 2 * width), BF16),
            pltpu.VMEM((2, part, 2 * width), BF16),
            pltpu.VMEM((2, rows // 2, na), F32),
            pltpu.VMEM((2, rows // 2, nbw), F32),
            pltpu.VMEM((2, rows // 2, na), BF16),
            pltpu.VMEM((2, rows // 2, nbw), BF16),
            pltpu.VMEM((2, rows // 2, na), BF16),
            pltpu.VMEM((2, rows // 2, nbw), BF16),
            pltpu.VMEM((rows, ff), BF16),
            pltpu.VMEM((ff, width), BF16),
            pltpu.VMEM((G - 1, part, width), BF16),
            pltpu.VMEM((2, part, width), BF16),
            pltpu.VMEM((2, part, width), BF16),
            pltpu.VMEM((part, width), F32),
            pltpu.VMEM((rows, LANE), F32),
            pltpu.VMEM((G, 8, rows), F32),
            pltpu.VMEM((G, 8, part), F32),
            dma((G + 7,)),
            dma((4, 2)),
            dma((2,)),
            dma((2,)),
            dma((2, PIECES)),
            dma((2, G - 1)),
            dma((2, G - 1, PIECES)),
            dma((1,)),
            dma((1,)),
            dma((2,)),
            dma((nt, 2)),
            dma((2,)),
            dma((nt, 2)),
            dma((2,)),
            dma((2, steps)),
            dma((2, 4)),
            dma((3, steps)),
            dma((G - 1,)),
            dma((2, width // TILE)),
            dma((2, width // TILE)),
            dma((2, G - 1)),
            dma((2, G - 1)),
        ],
        compiler_params=pltpu.CompilerParams(
            collective_id=0, has_side_effects=True, vmem_limit_bytes=63500000
        ),
    )(
        tokens,
        row(norm_gain),
        row(norm_bias),
        gate_weight,
        up_weight,
        gate_scale.reshape(-1, LANE),
        up_scale.reshape(-1, LANE),
        down_weight,
        row(down_scale),
        row(out_gain),
        row(out_bias),
    )


def local(*args):
    rows, width = args[0].shape
    ff = args[3].shape[1]
    fits = (
        lax.axis_size("cb") == G
        and lax.axis_size("ra") == G
        and lax.axis_size("dp") == 2
        and rows % (256 * G) == 0
        and width % TILE == 0
        and ff % TILE == 0
        and min(pair[1][1] for pair in tiles_of(ff)[2]) > 0
        and rows * width <= 1 << 20
        and ff * width <= 2816 * 1024
    )
    return (fused if fits else plain)(*args)


def solution(mesh):
    return jax.shard_map(
        local,
        mesh=mesh,
        in_specs=(
            P("dp", "cb"),
            P("cb"),
            P("cb"),
            P("cb", "ra"),
            P("cb", "ra"),
            P("ra"),
            P("ra"),
            P("ra", "cb"),
            P("cb"),
            P("cb"),
            P("cb"),
        ),
        out_specs=P(("dp", "ra"), "cb"),
        check_vma=False,
    )
```
